32 devices in a mesh: sp: 8 (over z, y), tp: 4 (over x, core).
Axes of the slice: x: 2, y: 2, z: 4, core: 2. Of those that a mesh axis runs over, the one named last changes fastest.
Arguments:
- resid: bfloat16 [12288, 2048], P(('sp', 'tp')), may hold values from -6 to 6
- cond: bfloat16 [2048], P('sp'), may hold values from -6 to 6
- mod_shift: bfloat16 [2048, 2048], P('sp', 'tp'), may hold values from -0.125 to 0.125
- mod_scale: bfloat16 [2048, 2048], P('sp', 'tp'), may hold values from -0.125 to 0.125
- mod_gate: bfloat16 [2048, 2048], P('sp', 'tp'), may hold values from -0.125 to 0.125
- norm_gain: float32 [2048], replicated, may hold values from 0.1 to 1.9
- context: bfloat16 [512, 2048], P('sp'), may hold values from -6 to 6
- w_query: bfloat16 [2048, 2048], P(None, 'tp'), may hold values from -0.125 to 0.125
- w_key: bfloat16 [2048, 2048], P(None, 'tp'), may hold values from -0.125 to 0.125
- w_value: bfloat16 [2048, 2048], P(None, 'tp'), may hold values from -0.125 to 0.125
- query_gain: float32 [128], replicated, may hold values from 0.5 to 6, as said below
- key_gain: float32 [128], replicated, may hold values from 0.5 to 6, as said below
- offset_bias: float32 [16, 15, 31], P('tp'), may hold values from -4 to 4
- context_bias: float32 [16], P('tp'), may hold values from -4.5 to 1
- w_out: bfloat16 [2048, 2048], replicated, may hold values from -0.5 to 0.5
Outputs:
- mixed: bfloat16 [12288, 2048], P(('sp', 'tp'))
The draws below stay inside these ranges and needn't reach their ends.
Inputs may be any that keep to these rules, and one draw needn't show every extreme that they name: `query_gain`: positive gains. `key_gain`: positive gains.
All inputs are finite; a program needn't handle non-finite values.
Results may differ from the reference program's by a relative error of at most 0.0085.
The reference program's roundings to bfloat16 on the way count: a program that leaves them out, or rounds other values in their place, can miss the bound.
Values may be sent and summed in bfloat16 or wider, within the bound.
No kernel may reach another device: no remote copies, remote signals or barrier semaphores. Data moves between devices by JAX's collectives and lax.ppermute only.
A program may use at most 128 MiB of HBM per device.

```python
import math
import jax
import jax.numpy as jnp
from jax import lax

D = 2048
HEADS = 16
HEAD_DIM = 128
GRID_W = 64
WIN_ROWS = 8
WIN_COLS = 16
ROWS = 192
TOKENS = 12288
CTX = 512


def draw_query_gain(key, part):
    local = jax.random.fold_in(key, 11)
    values = jax.random.uniform(local, (HEAD_DIM,), jnp.float32, 0.6, 1.4)
    return values


def draw_key_gain(key, part):
    local = jax.random.fold_in(key, 23)
    values = jax.random.uniform(local, (HEAD_DIM,), jnp.float32, 0.6, 1.4)
    return values


def draw_context_bias(key, part):
    local = jax.random.fold_in(key, 37)
    level = math.log(float(WIN_ROWS * WIN_COLS) / float(CTX))
    values = jax.random.uniform(local, (HEADS,), jnp.float32, -2.0, -0.5)
    return values + level


def levels(rng, dims, cuts, smallest, high):
    loudness, own = 1.0, jax.random.fold_in(rng, 6)
    for position, shards_of in cuts:
        draws = jnp.exp(jax.random.uniform(jax.random.fold_in(own, position), (shards_of,), jnp.float32, smallest / len(cuts), high / len(cuts)))
        loudness = loudness * jnp.repeat(draws, dims[position] // shards_of).reshape([-1 if axis == position else 1 for axis in range(len(dims))])
    return loudness


def scatter_about(key, extent, scale, most, cuts=(), kind=jnp.bfloat16):
    drawn = scale * jax.random.normal(key, extent, jnp.float32)
    if cuts:
        drawn = drawn * levels(key, extent, cuts, -0.22, 0.18)
    return jnp.clip(drawn, -most, most).astype(kind)


def setup_inputs(seed: int = 0) -> dict:
    streams_of = jax.random.split(jax.random.key(seed), 16)
    return {
        "resid": scatter_about(streams_of[0], (TOKENS, D), 1.0, 6.0, ((0, 32),)),
        "cond": scatter_about(streams_of[1], (D,), 1.0, 6.0, ((0, 8),)),
        "mod_shift": scatter_about(streams_of[2], (D, D), D ** -0.5, 0.125, ((0, 8), (1, 4))),
        "mod_scale": scatter_about(streams_of[3], (D, D), D ** -0.5, 0.125, ((0, 8), (1, 4))),
        "mod_gate": scatter_about(streams_of[4], (D, D), D ** -0.5, 0.125, ((0, 8), (1, 4))),
        "norm_gain": jnp.clip(1.0 + 0.18 * jax.random.normal(streams_of[5], (D,), jnp.float32), 0.1, 1.9),
        "context": scatter_about(streams_of[6], (CTX, D), 1.0, 6.0, ((0, 8),)),
        "w_query": scatter_about(streams_of[7], (D, HEADS * HEAD_DIM), D ** -0.5, 0.125, ((1, 4),)),
        "w_key": scatter_about(streams_of[8], (D, HEADS * HEAD_DIM), D ** -0.5, 0.125, ((1, 4),)),
        "w_value": scatter_about(streams_of[9], (D, HEADS * HEAD_DIM), D ** -0.5, 0.125, ((1, 4),)),
        "query_gain": draw_query_gain(jax.random.fold_in(streams_of[15], 71), 0),
        "key_gain": draw_key_gain(jax.random.fold_in(streams_of[15], 71), 0),
        "offset_bias": scatter_about(streams_of[12], (HEADS, 2 * WIN_ROWS - 1, 2 * WIN_COLS - 1), 1.0, 4.0, ((0, 4),), jnp.float32),
        "context_bias": draw_context_bias(jax.random.fold_in(streams_of[15], 71), 0),
        "w_out": scatter_about(streams_of[14], (HEADS * HEAD_DIM, D), (HEADS * HEAD_DIM // 16) ** -0.5, 0.5),
    }


EPS = 1e-06

def widen(values):
    return lax.optimization_barrier(values).astype(jnp.float32)

def normed_heads(values, gain):
    count = values.shape[0]
    split = values.reshape(count, HEADS, HEAD_DIM)
    scaled = split * lax.rsqrt(lax.optimization_barrier(jnp.mean(split * split, axis=-1, keepdims=True)) + EPS) * gain.astype(jnp.float32)
    return scaled.reshape(count, HEADS * HEAD_DIM).astype(jnp.bfloat16)

def reference(resid, cond, mod_shift, mod_scale, mod_gate, norm_gain, context, w_query, w_key, w_value, query_gain, key_gain, offset_bias, context_bias, w_out):
    lifted = jax.nn.silu(cond.astype(jnp.float32)).astype(jnp.bfloat16)
    shift = jnp.dot(lifted, mod_shift, preferred_element_type=jnp.float32)
    scale = jnp.dot(lifted, mod_scale, preferred_element_type=jnp.float32)
    gate = jnp.dot(lifted, mod_gate, preferred_element_type=jnp.float32)
    floats = resid.astype(jnp.float32)
    inverse = lax.rsqrt(lax.optimization_barrier(jnp.mean(floats * floats, axis=-1, keepdims=True)) + EPS)
    normed = (floats * inverse * norm_gain.astype(jnp.float32) * (1.0 + scale) + shift).astype(jnp.bfloat16)
    query = normed_heads(jnp.dot(normed, w_query, preferred_element_type=jnp.float32), query_gain)
    key = normed_heads(jnp.dot(normed, w_key, preferred_element_type=jnp.float32), key_gain)
    value = jnp.dot(normed, w_value, preferred_element_type=jnp.float32).astype(jnp.bfloat16)
    ctx_floats = context.astype(jnp.float32)
    ctx_inverse = lax.rsqrt(lax.optimization_barrier(jnp.mean(ctx_floats * ctx_floats, axis=-1, keepdims=True)) + EPS)
    ctx_normed = (ctx_floats * ctx_inverse * norm_gain.astype(jnp.float32)).astype(jnp.bfloat16)
    ctx_key = normed_heads(jnp.dot(ctx_normed, w_key, preferred_element_type=jnp.float32), key_gain)
    ctx_value = jnp.dot(ctx_normed, w_value, preferred_element_type=jnp.float32).astype(jnp.bfloat16)
    ctx_key = widen(ctx_key).reshape(CTX, HEADS, HEAD_DIM)
    ctx_value = widen(ctx_value).reshape(CTX, HEADS, HEAD_DIM)
    q_grid = widen(query).reshape(ROWS, GRID_W, HEADS, HEAD_DIM)
    k_grid = widen(key).reshape(ROWS, GRID_W, HEADS, HEAD_DIM)
    v_grid = widen(value).reshape(ROWS, GRID_W, HEADS, HEAD_DIM)
    columns = jnp.arange(GRID_W, dtype=jnp.int32)
    col_start = jnp.clip(columns - WIN_COLS // 2, 0, GRID_W - WIN_COLS)
    valid = (columns[None, :] >= col_start[:, None]) & (columns[None, :] < col_start[:, None] + WIN_COLS)
    col_offset = jnp.clip(columns[None, :] - columns[:, None] + WIN_COLS - 1, 0, 2 * WIN_COLS - 2)
    bias_table = offset_bias.astype(jnp.float32)
    ctx_shift = context_bias.astype(jnp.float32)[:, None, None]
    factor = HEAD_DIM ** (-0.5)

    def one_row(row):
        start = jnp.clip(row - WIN_ROWS // 2, 0, ROWS - WIN_ROWS).astype(jnp.int32)
        queries = lax.dynamic_index_in_dim(q_grid, row, 0, keepdims=False)
        keys = lax.dynamic_slice_in_dim(k_grid, start, WIN_ROWS, 0)
        values = lax.dynamic_slice_in_dim(v_grid, start, WIN_ROWS, 0)
        row_offset = (start + jnp.arange(WIN_ROWS, dtype=jnp.int32) - row + WIN_ROWS - 1).astype(jnp.int32)
        bias = bias_table[:, row_offset][:, :, col_offset]
        s_win = jnp.einsum('qhd,rkhd->hqrk', queries, keys) * factor + jnp.transpose(bias, (0, 2, 1, 3))
        s_win = jnp.where(valid[None, :, None, :], s_win, -1e+30).reshape(HEADS, GRID_W, WIN_ROWS * GRID_W)
        s_ctx = jnp.einsum('qhd,chd->hqc', queries, ctx_key) * factor + ctx_shift
        probs = jax.nn.softmax(jnp.concatenate([s_win, s_ctx], axis=-1), axis=-1).astype(jnp.bfloat16)
        probs = widen(probs)
        p_win = probs[:, :, :WIN_ROWS * GRID_W].reshape(HEADS, GRID_W, WIN_ROWS, GRID_W)
        p_ctx = probs[:, :, WIN_ROWS * GRID_W:]
        out = jnp.einsum('hqrk,rkhd->qhd', p_win, values) + jnp.einsum('hqc,chd->qhd', p_ctx, ctx_value)
        return out.astype(jnp.bfloat16).reshape(GRID_W, HEADS * HEAD_DIM)
    attended = lax.map(one_row, jnp.arange(ROWS, dtype=jnp.int32)).reshape(TOKENS, HEADS * HEAD_DIM)
    projected = jnp.dot(attended, w_out, preferred_element_type=jnp.float32)
    return (floats + gate * projected).astype(jnp.bfloat16)
```

```python
import functools
import math

import jax
import jax.numpy as jnp
from jax import lax
from jax.experimental import pallas as pl
from jax.experimental.pallas import tpu as pltpu
from jax.sharding import PartitionSpec as P

HEAD_DIM = 128
GRID_W = 64
WIN_ROWS = 8
WIN_COLS = 16
REACH = WIN_ROWS // 2
EPS = 1e-06
LOG2E = math.log2(math.e)
BLANK = 2 * WIN_ROWS
TABLES = BLANK + 1
F32 = jnp.float32
BF16 = jnp.bfloat16
MIB = 1 << 20

VM = pl.BlockSpec(memory_space=pltpu.VMEM)
SM = pl.BlockSpec(memory_space=pltpu.SMEM)


def params(mib):
    return pltpu.CompilerParams(vmem_limit_bytes=mib * MIB)


def cost(flops, nbytes, exps=0):
    return pl.CostEstimate(flops=int(flops), bytes_accessed=int(nbytes), transcendentals=int(exps))


def mod_kernel(cond_ref, shift_ref, scale_ref, gate_ref, out_ref):
    cond = cond_ref[...].astype(F32)
    lifted = (cond / (1.0 + jnp.exp(-cond))).astype(BF16)
    lifted = jnp.broadcast_to(lifted, (16, lifted.shape[1]))
    width = shift_ref.shape[1]
    for i, ref in enumerate((shift_ref, scale_ref, gate_ref)):
        part = jnp.dot(lifted, ref[...], preferred_element_type=F32)
        out_ref[:, i * width : (i + 1) * width] = part[:1]


def mod_part(cond, mod_shift, mod_scale, mod_gate):
    rows, width = mod_shift.shape
    return pl.pallas_call(
        mod_kernel,
        out_shape=jax.ShapeDtypeStruct((1, 3 * width), F32),
        in_specs=[VM] * 4,
        out_specs=VM,
        name="mod_part",
        compiler_params=params(8),
        cost_estimate=cost(96 * rows * width, 6 * rows * width),
    )(cond.reshape(1, -1), mod_shift, mod_scale, mod_gate)


def place_kernel(count, spots_ref, *refs):
    pieces, gain_ref, out_ref = refs[:count], refs[count], refs[count + 1]
    width = pieces[0].shape[1] // 3
    for i, piece in enumerate(pieces):
        spot = pl.multiple_of(spots_ref[i] * width, width)
        gain = gain_ref[:, pl.ds(spot, width)]
        out_ref[0:1, pl.ds(spot, width)] = piece[:, :width]
        out_ref[1:2, pl.ds(spot, width)] = gain * (1.0 + piece[:, width : 2 * width])
        out_ref[2:3, pl.ds(spot, width)] = piece[:, 2 * width :]


def place_mods(pieces, spots, norm_gain):
    depth = norm_gain.shape[0]
    return pl.pallas_call(
        functools.partial(place_kernel, len(pieces)),
        out_shape=jax.ShapeDtypeStruct((8, depth), F32),
        in_specs=[SM] + [VM] * (len(pieces) + 1),
        out_specs=VM,
        name="place_mods",
        compiler_params=params(4),
        cost_estimate=cost(1 << 20, 1 << 16),
    )(spots, *pieces, norm_gain.reshape(1, -1))


def table_kernel(bias_ref, out_ref):
    heads = out_ref.shape[0]
    column = lax.broadcasted_iota(jnp.int32, (GRID_W, 2 * GRID_W), 0)
    lane = lax.broadcasted_iota(jnp.int32, (GRID_W, 2 * GRID_W), 1)
    left = lane < GRID_W
    begin = jnp.clip(column - WIN_COLS // 2, 0, GRID_W - WIN_COLS)
    key = jnp.where(left, lane, lane - GRID_W)
    valid = (key >= begin) & (key < begin + WIN_COLS)
    empty = jnp.full((GRID_W, 2 * GRID_W), -1e30, F32)
    for h in range(heads):
        rolled = []
        for d in range(2 * WIN_ROWS - 1):
            row = jnp.broadcast_to(bias_ref[h, d : d + 1, :] * LOG2E, (GRID_W, 2 * GRID_W))
            lo = pltpu.roll(row, 2 * GRID_W - WIN_COLS + 1, 1, stride=1, stride_axis=0)
            hi = pltpu.roll(row, GRID_W - WIN_COLS + 1, 1, stride=1, stride_axis=0)
            rolled.append((jnp.where(valid & left, lo, empty), jnp.where(valid & ~left, hi, empty)))
        for d in range(2 * WIN_ROWS - 2):
            out_ref[h, d] = jnp.where(left, rolled[d][0], rolled[d + 1][1])
        out_ref[h, 2 * WIN_ROWS - 2] = rolled[WIN_ROWS + 2][0]
        out_ref[h, 2 * WIN_ROWS - 1] = rolled[WIN_ROWS - REACH - 1][1]
        out_ref[h, BLANK] = empty


def bias_tables(offset_bias):
    heads, rows, cols = offset_bias.shape
    padded = jnp.pad(offset_bias, ((0, 0), (0, 16 - rows), (0, 2 * GRID_W - cols)))
    return pl.pallas_call(
        table_kernel,
        out_shape=jax.ShapeDtypeStruct((heads, TABLES, GRID_W, 2 * GRID_W), F32),
        in_specs=[VM],
        out_specs=VM,
        name="bias_tables",
        compiler_params=params(8),
        cost_estimate=cost(1 << 22, heads * TABLES * GRID_W * 2 * GRID_W * 4),
    )(padded)


def normed_heads(values, gain, heads):
    parts = []
    for h in range(heads):
        part = values[:, h * HEAD_DIM : (h + 1) * HEAD_DIM]
        square = jnp.mean(part * part, axis=-1, keepdims=True)
        parts.append((part * lax.rsqrt(square + EPS) * gain).astype(BF16))
    return jnp.concatenate(parts, axis=1)


def qkv_kernel(count, heads, tile, *refs):
    pieces = refs[:count]
    mods_ref, wq_ref, wk_ref, wv_ref, qg_ref, kg_ref, q_ref, kv_ref, normed = refs[count:]
    width = heads * HEAD_DIM
    strip = 16
    shift, gain = mods_ref[0:1, :], mods_ref[1:2, :]
    base = 0
    for piece in pieces:

        def one(i, _, piece=piece, base=base):
            at = pl.multiple_of(i * strip, strip)
            floats = piece[pl.ds(at, strip), :].astype(F32)
            inverse = lax.rsqrt(jnp.mean(floats * floats, axis=-1, keepdims=True) + EPS)
            normed[pl.ds(base + at, strip), :] = (floats * inverse * gain + shift).astype(BF16)
            return 0

        lax.fori_loop(0, piece.shape[0] // strip, one, 0, unroll=2)
        base += piece.shape[0]

    def project(i, _):
        rows = pl.ds(pl.multiple_of(i * tile, tile), tile)
        x = normed[rows, :]
        q_ref[rows, :] = normed_heads(
            jnp.dot(x, wq_ref[...], preferred_element_type=F32), qg_ref[...], heads
        )
        kv_ref[rows, :width] = normed_heads(
            jnp.dot(x, wk_ref[...], preferred_element_type=F32), kg_ref[...], heads
        )
        kv_ref[rows, width:] = jnp.dot(x, wv_ref[...], preferred_element_type=F32).astype(BF16)
        return 0

    lax.fori_loop(0, base // tile, project, 0)


def qkv(pieces, mods, w_query, w_key, w_value, query_gain, key_gain, heads):
    total = sum(p.shape[0] for p in pieces)
    depth, width = w_query.shape
    tile = 256 if total % 256 == 0 else 128
    return pl.pallas_call(
        functools.partial(qkv_kernel, len(pieces), heads, tile),
        out_shape=(
            jax.ShapeDtypeStruct((total, width), BF16),
            jax.ShapeDtypeStruct((total, 2 * width), BF16),
        ),
        in_specs=[VM] * (len(pieces) + 6),
        out_specs=(VM, VM),
        scratch_shapes=[pltpu.VMEM((total, depth), BF16)],
        name="qkv",
        compiler_params=params(40),
        cost_estimate=cost(6 * total * depth * width, total * depth * 2 + 6 * depth * width),
    )(*pieces, mods, w_query, w_key, w_value, query_gain.reshape(1, -1), key_gain.reshape(1, -1))


def context_kernel(heads, x_ref, gain_ref, wk_ref, wv_ref, kg_ref, kv_ref):
    width = heads * HEAD_DIM
    floats = x_ref[...].astype(F32)
    inverse = lax.rsqrt(jnp.mean(floats * floats, axis=-1, keepdims=True) + EPS)
    x = (floats * inverse * gain_ref[...]).astype(BF16)
    kv_ref[:, :width] = normed_heads(
        jnp.dot(x, wk_ref[...], preferred_element_type=F32), kg_ref[...], heads
    )
    kv_ref[:, width:] = jnp.dot(x, wv_ref[...], preferred_element_type=F32).astype(BF16)


def context_kv(context, norm_gain, w_key, w_value, key_gain, heads):
    count, depth = context.shape
    width = w_key.shape[1]
    return pl.pallas_call(
        functools.partial(context_kernel, heads),
        out_shape=jax.ShapeDtypeStruct((count, 2 * width), BF16),
        in_specs=[VM] * 5,
        out_specs=VM,
        name="context_kv",
        compiler_params=params(16),
        cost_estimate=cost(4 * count * depth * width, 4 * depth * width),
    )(context, norm_gain.reshape(1, -1), w_key, w_value, key_gain.reshape(1, -1))


def attend_kernel(heads, span, groups, counts, meta_ref, cbias_ref, *refs):
    n_q, n_kv, n_ctx = counts
    q_refs, refs = refs[:n_q], refs[n_q:]
    kv_refs, refs = refs[:n_kv], refs[n_kv:]
    ctx_refs, refs = refs[:n_ctx], refs[n_ctx:]
    tab_ref, out_ref, keys, queries, context, scores, weights = refs
    width = heads * HEAD_DIM
    block = span * GRID_W
    key_rows = span + WIN_ROWS
    window = key_rows * GRID_W
    ctx_count = context.shape[0]
    factor = LOG2E * HEAD_DIM**-0.5
    lines = 2 * GRID_W
    for i, ref in enumerate(kv_refs):
        at = pl.multiple_of((meta_ref[2 + i] + REACH) * GRID_W, GRID_W)
        keys[pl.ds(at, ref.shape[0]), :] = ref[...]
    at = 0
    for ref in q_refs:
        queries[at : at + ref.shape[0], :] = ref[...]
        at += ref.shape[0]
    at = 0
    for ref in ctx_refs:
        context[at : at + ref.shape[0], :] = ref[...]
        at += ref.shape[0]
    first, total = meta_ref[0], meta_ref[1]
    nt = (((1,), (1,)), ((), ()))

    def group(i, _):
        row = meta_ref[2 + n_kv + 2 * i]
        q_at = pl.multiple_of(meta_ref[3 + n_kv + 2 * i], GRID_W)
        top = first + row
        start = jnp.clip(top - REACH, 0, total - key_rows)
        k_at = pl.multiple_of((start - first + REACH) * GRID_W, GRID_W)
        spots = []
        for r in range(span):
            g = top + r
            a = jnp.clip(g - REACH, 0, total - WIN_ROWS)
            for p in range(key_rows // 2):
                u = start + 2 * p
                lv = (u >= a) & (u < a + WIN_ROWS)
                rv = (u + 1 >= a) & (u + 1 < a + WIN_ROWS)
                both = jnp.where(rv, u - g + WIN_ROWS - 1, BLANK - 2)
                spots.append(jnp.where(lv, both, jnp.where(rv, BLANK - 1, BLANK)))
        out_at = pl.multiple_of(i * block, block)
        for h in range(heads):
            hk = slice(h * HEAD_DIM, (h + 1) * HEAD_DIM)
            hv = slice(width + h * HEAD_DIM, width + (h + 1) * HEAD_DIM)
            q = queries[pl.ds(q_at, block), hk]
            scores[h, :, :window] = lax.dot_general(
                q, keys[pl.ds(k_at, window), hk], nt, preferred_element_type=F32
            )
            scores[h, :, window:] = lax.dot_general(
                q, context[:, hk], nt, preferred_element_type=F32
            )
            cbias = cbias_ref[h] * LOG2E
            sums = []
            for r in range(span):
                rows = slice(r * GRID_W, (r + 1) * GRID_W)
                tops = None
                for p in range(key_rows // 2):
                    cols = slice(p * lines, (p + 1) * lines)
                    tile = scores[h, rows, cols] * factor
                    tile = tile + tab_ref[h, spots[r * (key_rows // 2) + p]]
                    scores[h, rows, cols] = tile
                    tops = tile if tops is None else jnp.maximum(tops, tile)
                ctx = scores[h, rows, window : window + lines]
                for p in range(1, ctx_count // lines):
                    cols = slice(window + p * lines, window + (p + 1) * lines)
                    ctx = jnp.maximum(ctx, scores[h, rows, cols])
                tops = jnp.maximum(tops, ctx * factor + cbias)
                high = jnp.max(tops, axis=1, keepdims=True)
                acc = None
                for p in range(key_rows // 2 + ctx_count // lines):
                    cols = slice(p * lines, (p + 1) * lines)
                    tile = scores[h, rows, cols]
                    if p < key_rows // 2:
                        tile = jnp.exp2(tile - high)
                    else:
                        tile = jnp.exp2(tile * factor - (high - cbias))
                    acc = tile if acc is None else acc + tile
                    weights[h, rows, cols] = tile.astype(BF16)
                sums.append(jnp.sum(acc, axis=1, keepdims=True))
            out = jnp.dot(
                weights[h, :, :window], keys[pl.ds(k_at, window), hv], preferred_element_type=F32
            )
            out = out + jnp.dot(
                weights[h, :, window:], context[:, hv], preferred_element_type=F32
            )
            out = out / jnp.concatenate(sums, axis=0)
            out_ref[pl.ds(out_at, block), hk] = out.astype(BF16)
        return 0

    lax.fori_loop(0, groups, group, 0)


def attend(queries, kvs, ctx, tables, context_bias, meta, span, groups, rows):
    heads = tables.shape[0]
    width = heads * HEAD_DIM
    block = span * GRID_W
    ctx_count = sum(c.shape[0] for c in ctx)
    keys = (span + WIN_ROWS) * GRID_W + ctx_count
    q_rows = sum(q.shape[0] for q in queries)
    elements = groups * block * heads * keys
    return pl.pallas_call(
        functools.partial(
            attend_kernel, heads, span, groups, (len(queries), len(kvs), len(ctx))
        ),
        out_shape=jax.ShapeDtypeStruct((groups * block, width), BF16),
        in_specs=[SM, SM] + [VM] * (len(queries) + len(kvs) + len(ctx) + 1),
        out_specs=VM,
        scratch_shapes=[
            pltpu.VMEM(((rows + 2 * REACH) * GRID_W, 2 * width), BF16),
            pltpu.VMEM((q_rows, width), BF16),
            pltpu.VMEM((ctx_count, 2 * width), BF16),
            pltpu.VMEM((heads, block, keys), F32),
            pltpu.VMEM((heads, block, keys), BF16),
        ],
        name="attend",
        compiler_params=params(40),
        cost_estimate=cost(8 * elements * HEAD_DIM, 8 << 20, elements),
    )(meta, context_bias, *queries, *kvs, *ctx, tables)


def out_kernel(count, tile, spots_ref, *refs):
    pieces = refs[:count]
    w_ref, resid_ref, mods_ref, out_ref = refs[count:]
    depth = pieces[0].shape[1]

    def one(i, _):
        cols = pl.ds(pl.multiple_of(i * tile, tile), tile)
        total = None
        for j, piece in enumerate(pieces):
            rows = pl.ds(pl.multiple_of(spots_ref[j] * depth, depth), depth)
            part = jnp.dot(piece[...], w_ref[rows, cols], preferred_element_type=F32)
            total = part if total is None else total + part
        gate = mods_ref[2:3, cols]
        out_ref[:, cols] = (resid_ref[:, cols].astype(F32) + gate * total).astype(BF16)
        return 0

    lax.fori_loop(0, w_ref.shape[1] // tile, one, 0)


def out_project(pieces, spots, w_out, resid, mods):
    count, width = resid.shape
    return pl.pallas_call(
        functools.partial(out_kernel, len(pieces), 256),
        out_shape=jax.ShapeDtypeStruct((count, width), BF16),
        in_specs=[SM] + [VM] * (len(pieces) + 3),
        out_specs=VM,
        name="out_project",
        compiler_params=params(24),
        cost_estimate=cost(2 * count * width * w_out.shape[0], w_out.size * 2 + 4 * resid.size),
    )(spots, *pieces, w_out, resid, mods)


def swap(count, bit):
    return [(i, i ^ bit) for i in range(count)]


def shards(
    resid,
    cond,
    mod_shift,
    mod_scale,
    mod_gate,
    norm_gain,
    context,
    w_query,
    w_key,
    w_value,
    query_gain,
    key_gain,
    offset_bias,
    context_bias,
    w_out,
):
    heads = offset_bias.shape[0]
    sp, tp = lax.axis_size("sp"), lax.axis_size("tp")
    me_s, me_t = lax.axis_index("sp"), lax.axis_index("tp")
    own = resid.shape[0]
    tokens = own * tp
    rows = tokens // GRID_W

    part = mod_part(cond, mod_shift, mod_scale, mod_gate)
    bit = 1
    while bit < sp:
        part = part + lax.ppermute(part, "sp", swap(sp, bit))
        bit *= 2
    parts = [part]
    bit = 1
    while bit < tp:
        parts += [lax.ppermute(p, "tp", swap(tp, bit)) for p in parts]
        bit *= 2
    spots = me_t ^ jnp.arange(tp, dtype=jnp.int32)
    mods = place_mods(parts, spots, norm_gain)

    tables = bias_tables(offset_bias)
    ctx = lax.all_gather(
        context_kv(context, norm_gain, w_key, w_value, key_gain, heads), "sp", axis=0, tiled=True
    )
    piece = lax.all_gather(resid, "tp", axis=0, tiled=True)
    q, kv = qkv([piece], mods, w_query, w_key, w_value, query_gain, key_gain, heads)

    edge = REACH * GRID_W
    above = lax.ppermute(kv[tokens - edge :], "sp", [(i, i + 1) for i in range(sp - 1)])
    below = lax.ppermute(kv[:edge], "sp", [(i + 1, i) for i in range(sp - 1)])
    span = 4 if rows % 4 == 0 else 2
    groups = rows // span
    meta = [me_s * rows, sp * rows, 0, -REACH, rows]
    for i in range(groups):
        meta += [i * span, i * span * GRID_W]
    meta = jnp.stack([jnp.asarray(m, jnp.int32) for m in meta])
    attended = attend(
        [q], [kv, above, below], [ctx], tables, context_bias, meta, span, groups, rows
    )
    full = lax.all_to_all(attended.reshape(tp, own, -1), "tp", split_axis=0, concat_axis=0)
    return out_project(
        [full[i] for i in range(tp)], jnp.arange(tp, dtype=jnp.int32), w_out, resid, mods
    )


def solution(mesh):
    in_specs = (
        P(("sp", "tp"), None),
        P("sp"),
        P("sp", "tp"),
        P("sp", "tp"),
        P("sp", "tp"),
        P(),
        P("sp", None),
        P(None, "tp"),
        P(None, "tp"),
        P(None, "tp"),
        P(),
        P(),
        P("tp", None, None),
        P("tp"),
        P(),
    )
    out_specs = P(("sp", "tp"), None)
    return jax.shard_map(shards, mesh=mesh, in_specs=in_specs, out_specs=out_specs, check_vma=False)
```

```python
import functools
import math

import jax
import jax.numpy as jnp
from jax import lax
from jax.experimental import pallas as pl
from jax.experimental.pallas import tpu as pltpu
from jax.sharding import PartitionSpec as P


HEAD_DIM = 128
GRID_W = 64
WIN_ROWS = 8
WIN_COLS = 16
REACH = WIN_ROWS // 2
EPS = 1e-06
LOG2E = math.log2(math.e)
BLANK = 2 * WIN_ROWS
TABLES = BLANK + 1
F32 = jnp.float32
BF16 = jnp.bfloat16
MIB = 1 << 20

VM = pl.BlockSpec(memory_space=pltpu.VMEM)
SM = pl.BlockSpec(memory_space=pltpu.SMEM)


def params(mib):
    return pltpu.CompilerParams(vmem_limit_bytes=mib * MIB)


def cost(flops, nbytes, exps=0):
    return pl.CostEstimate(flops=int(flops), bytes_accessed=int(nbytes), transcendentals=int(exps))


def mod_kernel(cond_ref, shift_ref, scale_ref, gate_ref, out_ref):
    cond = cond_ref[...].astype(F32)
    lifted = (cond / (1.0 + jnp.exp(-cond))).astype(BF16)
    lifted = jnp.broadcast_to(lifted, (16, lifted.shape[1]))
    width = shift_ref.shape[1]
    for i, ref in enumerate((shift_ref, scale_ref, gate_ref)):
        part = jnp.dot(lifted, ref[...], preferred_element_type=F32)
        out_ref[:, i * width : (i + 1) * width] = part[:1]


def mod_part(cond, mod_shift, mod_scale, mod_gate):
    rows, width = mod_shift.shape
    return pl.pallas_call(
        mod_kernel,
        out_shape=jax.ShapeDtypeStruct((1, 3 * width), F32),
        in_specs=[VM] * 4,
        out_specs=VM,
        name="mod_part",
        compiler_params=params(8),
        cost_estimate=cost(96 * rows * width, 6 * rows * width),
    )(cond.reshape(1, -1), mod_shift, mod_scale, mod_gate)


def place_kernel(count, spots_ref, *refs):
    pieces, gain_ref, out_ref = refs[:count], refs[count], refs[count + 1]
    width = pieces[0].shape[1] // 3
    for i, piece in enumerate(pieces):
        spot = pl.multiple_of(spots_ref[i] * width, width)
        gain = gain_ref[:, pl.ds(spot, width)]
        out_ref[0:1, pl.ds(spot, width)] = piece[:, :width]
        out_ref[1:2, pl.ds(spot, width)] = gain * (1.0 + piece[:, width : 2 * width])
        out_ref[2:3, pl.ds(spot, width)] = piece[:, 2 * width :]


def place_mods(pieces, spots, norm_gain):
    depth = norm_gain.shape[0]
    return pl.pallas_call(
        functools.partial(place_kernel, len(pieces)),
        out_shape=jax.ShapeDtypeStruct((8, depth), F32),
        in_specs=[SM] + [VM] * (len(pieces) + 1),
        out_specs=VM,
        name="place_mods",
        compiler_params=params(4),
        cost_estimate=cost(1 << 20, 1 << 16),
    )(spots, *pieces, norm_gain.reshape(1, -1))


def table_kernel(bias_ref, out_ref):
    heads = out_ref.shape[0]
    column = lax.broadcasted_iota(jnp.int32, (GRID_W, 2 * GRID_W), 0)
    lane = lax.broadcasted_iota(jnp.int32, (GRID_W, 2 * GRID_W), 1)
    left = lane < GRID_W
    begin = jnp.clip(column - WIN_COLS // 2, 0, GRID_W - WIN_COLS)
    key = jnp.where(left, lane, lane - GRID_W)
    valid = (key >= begin) & (key < begin + WIN_COLS)
    empty = jnp.full((GRID_W, 2 * GRID_W), -1e30, F32)
    for h in range(heads):
        rolled = []
        for d in range(2 * WIN_ROWS - 1):
            row = jnp.broadcast_to(bias_ref[h, d : d + 1, :] * LOG2E, (GRID_W, 2 * GRID_W))
            lo = pltpu.roll(row, 2 * GRID_W - WIN_COLS + 1, 1, stride=1, stride_axis=0)
            hi = pltpu.roll(row, GRID_W - WIN_COLS + 1, 1, stride=1, stride_axis=0)
            rolled.append((jnp.where(valid & left, lo, empty), jnp.where(valid & ~left, hi, empty)))
        for d in range(2 * WIN_ROWS - 2):
            out_ref[h, d] = jnp.where(left, rolled[d][0], rolled[d + 1][1])
        out_ref[h, 2 * WIN_ROWS - 2] = rolled[WIN_ROWS + 2][0]
        out_ref[h, 2 * WIN_ROWS - 1] = rolled[WIN_ROWS - REACH - 1][1]
        out_ref[h, BLANK] = empty


def bias_tables(offset_bias):
    heads, rows, cols = offset_bias.shape
    padded = jnp.pad(offset_bias, ((0, 0), (0, 16 - rows), (0, 2 * GRID_W - cols)))
    return pl.pallas_call(
        table_kernel,
        out_shape=jax.ShapeDtypeStruct((heads, TABLES, GRID_W, 2 * GRID_W), F32),
        in_specs=[VM],
        out_specs=VM,
        name="bias_tables",
        compiler_params=params(8),
        cost_estimate=cost(1 << 22, heads * TABLES * GRID_W * 2 * GRID_W * 4),
    )(padded)


def normed_heads(values, gain, heads):
    parts = []
    for h in range(heads):
        part = values[:, h * HEAD_DIM : (h + 1) * HEAD_DIM]
        square = jnp.mean(part * part, axis=-1, keepdims=True)
        parts.append((part * lax.rsqrt(square + EPS) * gain).astype(BF16))
    return jnp.concatenate(parts, axis=1)


def qkv_kernel(count, heads, tile, *refs):
    pieces = refs[:count]
    mods_ref, wq_ref, wk_ref, wv_ref, qg_ref, kg_ref, q_ref, kv_ref, normed = refs[count:]
    width = heads * HEAD_DIM
    strip = 16
    shift, gain = mods_ref[0:1, :], mods_ref[1:2, :]
    base = 0
    for piece in pieces:

        def one(i, _, piece=piece, base=base):
            at = pl.multiple_of(i * strip, strip)
            floats = piece[pl.ds(at, strip), :].astype(F32)
            inverse = lax.rsqrt(jnp.mean(floats * floats, axis=-1, keepdims=True) + EPS)
            normed[pl.ds(base + at, strip), :] = (floats * inverse * gain + shift).astype(BF16)
            return 0

        lax.fori_loop(0, piece.shape[0] // strip, one, 0, unroll=2)
        base += piece.shape[0]

    def project(i, _):
        rows = pl.ds(pl.multiple_of(i * tile, tile), tile)
        x = normed[rows, :]
        q_ref[rows, :] = normed_heads(
            jnp.dot(x, wq_ref[...], preferred_element_type=F32), qg_ref[...], heads
        )
        kv_ref[rows, :width] = normed_heads(
            jnp.dot(x, wk_ref[...], preferred_element_type=F32), kg_ref[...], heads
        )
        kv_ref[rows, width:] = jnp.dot(x, wv_ref[...], preferred_element_type=F32).astype(BF16)
        return 0

    lax.fori_loop(0, base // tile, project, 0)


def qkv(pieces, mods, w_query, w_key, w_value, query_gain, key_gain, heads):
    total = sum(p.shape[0] for p in pieces)
    depth, width = w_query.shape
    tile = 256 if total % 256 == 0 else 128
    return pl.pallas_call(
        functools.partial(qkv_kernel, len(pieces), heads, tile),
        out_shape=(
            jax.ShapeDtypeStruct((total, width), BF16),
            jax.ShapeDtypeStruct((total, 2 * width), BF16),
        ),
        in_specs=[VM] * (len(pieces) + 6),
        out_specs=(VM, VM),
        scratch_shapes=[pltpu.VMEM((total, depth), BF16)],
        name="qkv",
        compiler_params=params(40),
        cost_estimate=cost(6 * total * depth * width, total * depth * 2 + 6 * depth * width),
    )(*pieces, mods, w_query, w_key, w_value, query_gain.reshape(1, -1), key_gain.reshape(1, -1))


def context_kernel(heads, x_ref, gain_ref, wk_ref, wv_ref, kg_ref, kv_ref):
    width = heads * HEAD_DIM
    floats = x_ref[...].astype(F32)
    inverse = lax.rsqrt(jnp.mean(floats * floats, axis=-1, keepdims=True) + EPS)
    x = (floats * inverse * gain_ref[...]).astype(BF16)
    kv_ref[:, :width] = normed_heads(
        jnp.dot(x, wk_ref[...], preferred_element_type=F32), kg_ref[...], heads
    )
    kv_ref[:, width:] = jnp.dot(x, wv_ref[...], preferred_element_type=F32).astype(BF16)


def context_kv(context, norm_gain, w_key, w_value, key_gain, heads):
    count, depth = context.shape
    width = w_key.shape[1]
    return pl.pallas_call(
        functools.partial(context_kernel, heads),
        out_shape=jax.ShapeDtypeStruct((count, 2 * width), BF16),
        in_specs=[VM] * 5,
        out_specs=VM,
        name="context_kv",
        compiler_params=params(16),
        cost_estimate=cost(4 * count * depth * width, 4 * depth * width),
    )(context, norm_gain.reshape(1, -1), w_key, w_value, key_gain.reshape(1, -1))


def attend_kernel(heads, span, groups, q_spec, kv_spec, n_ctx, meta_ref, cbias_ref, *refs):
    n_q, n_kv = q_spec[-1][0] + 1, kv_spec[-1][0] + 1
    q_refs, refs = refs[:n_q], refs[n_q:]
    kv_refs, refs = refs[:n_kv], refs[n_kv:]
    ctx_refs, refs = refs[:n_ctx], refs[n_ctx:]
    tab_ref, out_ref, keys, queries, context, scores, weights = refs
    width = heads * HEAD_DIM
    block = span * GRID_W
    key_rows = span + WIN_ROWS
    window = key_rows * GRID_W
    ctx_count = context.shape[0]
    factor = LOG2E * HEAD_DIM**-0.5
    lines = 2 * GRID_W
    base = 2
    for i, (j, at, size) in enumerate(q_spec):
        to = pl.multiple_of(meta_ref[base + i] * GRID_W, GRID_W)
        queries[pl.ds(to, size), :] = q_refs[j][at : at + size, :]
    base += len(q_spec)
    for i, (j, at, size) in enumerate(kv_spec):
        to = pl.multiple_of((meta_ref[base + i] + REACH) * GRID_W, GRID_W)
        keys[pl.ds(to, size), :] = kv_refs[j][at : at + size, :]
    base += len(kv_spec)
    at = 0
    for ref in ctx_refs:
        context[at : at + ref.shape[0], :] = ref[...]
        at += ref.shape[0]
    first, total = meta_ref[0], meta_ref[1]
    nt = (((1,), (1,)), ((), ()))

    def group(i, _):
        row = meta_ref[base + i]
        q_at = pl.multiple_of(row * GRID_W, GRID_W)
        top = first + row
        start = jnp.clip(top - REACH, 0, total - key_rows)
        k_at = pl.multiple_of((start - first + REACH) * GRID_W, GRID_W)
        spots = []
        for r in range(span):
            g = top + r
            a = jnp.clip(g - REACH, 0, total - WIN_ROWS)
            for p in range(key_rows // 2):
                u = start + 2 * p
                lv = (u >= a) & (u < a + WIN_ROWS)
                rv = (u + 1 >= a) & (u + 1 < a + WIN_ROWS)
                both = jnp.where(rv, u - g + WIN_ROWS - 1, BLANK - 2)
                spots.append(jnp.where(lv, both, jnp.where(rv, BLANK - 1, BLANK)))
        for h in range(heads):
            hk = slice(h * HEAD_DIM, (h + 1) * HEAD_DIM)
            hv = slice(width + h * HEAD_DIM, width + (h + 1) * HEAD_DIM)
            q = queries[pl.ds(q_at, block), hk]
            scores[h, :, :window] = lax.dot_general(
                q, keys[pl.ds(k_at, window), hk], nt, preferred_element_type=F32
            )
            scores[h, :, window:] = lax.dot_general(
                q, context[:, hk], nt, preferred_element_type=F32
            )
            cbias = cbias_ref[h] * LOG2E
            sums = []
            for r in range(span):
                rows = slice(r * GRID_W, (r + 1) * GRID_W)
                tops = None
                for p in range(key_rows // 2):
                    cols = slice(p * lines, (p + 1) * lines)
                    tile = scores[h, rows, cols] * factor
                    tile = tile + tab_ref[h, spots[r * (key_rows // 2) + p]]
                    scores[h, rows, cols] = tile
                    tops = tile if tops is None else jnp.maximum(tops, tile)
                ctx = scores[h, rows, window : window + lines]
                for p in range(1, ctx_count // lines):
                    cols = slice(window + p * lines, window + (p + 1) * lines)
                    ctx = jnp.maximum(ctx, scores[h, rows, cols])
                tops = jnp.maximum(tops, ctx * factor + cbias)
                high = jnp.max(tops, axis=1, keepdims=True)
                acc = None
                for p in range(key_rows // 2 + ctx_count // lines):
                    cols = slice(p * lines, (p + 1) * lines)
                    tile = scores[h, rows, cols]
                    if p < key_rows // 2:
                        tile = jnp.exp2(tile - high)
                    else:
                        tile = jnp.exp2(tile * factor - (high - cbias))
                    acc = tile if acc is None else acc + tile
                    weights[h, rows, cols] = tile.astype(BF16)
                sums.append(jnp.sum(acc, axis=1, keepdims=True))
            out = jnp.dot(
                weights[h, :, :window], keys[pl.ds(k_at, window), hv], preferred_element_type=F32
            )
            out = out + jnp.dot(
                weights[h, :, window:], context[:, hv], preferred_element_type=F32
            )
            out = (out / jnp.concatenate(sums, axis=0)).astype(BF16)
            for r in range(span):
                to = pl.multiple_of(meta_ref[base + groups + i * span + r] * GRID_W, GRID_W)
                out_ref[pl.ds(to, GRID_W), hk] = out[r * GRID_W : (r + 1) * GRID_W]
        return 0

    lax.fori_loop(0, groups, group, 0)


def attend(queries, q_spec, kvs, kv_spec, ctx, tables, context_bias, meta, span, groups, rows):
    heads = tables.shape[0]
    width = heads * HEAD_DIM
    block = span * GRID_W
    ctx_count = sum(c.shape[0] for c in ctx)
    keys = (span + WIN_ROWS) * GRID_W + ctx_count
    elements = groups * block * heads * keys
    meta = jnp.stack([jnp.asarray(m, jnp.int32) for m in meta])
    return pl.pallas_call(
        functools.partial(attend_kernel, heads, span, groups, q_spec, kv_spec, len(ctx)),
        out_shape=jax.ShapeDtypeStruct((groups * block, width), BF16),
        in_specs=[SM, SM] + [VM] * (len(queries) + len(kvs) + len(ctx) + 1),
        out_specs=VM,
        scratch_shapes=[
            pltpu.VMEM(((rows + 2 * REACH) * GRID_W, 2 * width), BF16),
            pltpu.VMEM((rows * GRID_W, width), BF16),
            pltpu.VMEM((ctx_count, 2 * width), BF16),
            pltpu.VMEM((heads, block, keys), F32),
            pltpu.VMEM((heads, block, keys), BF16),
        ],
        name="attend",
        compiler_params=params(40),
        cost_estimate=cost(8 * elements * HEAD_DIM, 8 << 20, elements),
    )(meta, context_bias, *queries, *kvs, *ctx, tables)


def out_kernel(count, tile, spots_ref, *refs):
    pieces = refs[:count]
    w_ref, resid_ref, mods_ref, out_ref = refs[count:]
    depth = pieces[0].shape[1]

    def one(i, _):
        cols = pl.ds(pl.multiple_of(i * tile, tile), tile)
        total = None
        for j, piece in enumerate(pieces):
            rows = pl.ds(pl.multiple_of(spots_ref[j] * depth, depth), depth)
            part = jnp.dot(piece[...], w_ref[rows, cols], preferred_element_type=F32)
            total = part if total is None else total + part
        gate = mods_ref[2:3, cols]
        out_ref[:, cols] = (resid_ref[:, cols].astype(F32) + gate * total).astype(BF16)
        return 0

    lax.fori_loop(0, w_ref.shape[1] // tile, one, 0)


def out_project(pieces, spots, w_out, resid, mods):
    count, width = resid.shape
    return pl.pallas_call(
        functools.partial(out_kernel, len(pieces), 256),
        out_shape=jax.ShapeDtypeStruct((count, width), BF16),
        in_specs=[SM] + [VM] * (len(pieces) + 3),
        out_specs=VM,
        name="out_project",
        compiler_params=params(24),
        cost_estimate=cost(2 * count * width * w_out.shape[0], w_out.size * 2 + 4 * resid.size),
    )(spots, *pieces, w_out, resid, mods)


def swap(count, bit):
    return [(i, i ^ bit) for i in range(count)]


def tie(value, other):
    return lax.optimization_barrier((value, other))[0]


def plain(resid, mods, ctx, tables, weights, gains, context_bias, w_out, heads):
    sp, tp = lax.axis_size("sp"), lax.axis_size("tp")
    me_s = lax.axis_index("sp")
    own = resid.shape[0]
    tokens = own * tp
    rows = tokens // GRID_W
    piece = lax.all_gather(resid, "tp", axis=0, tiled=True)
    q, kv = qkv([piece], mods, *weights, *gains, heads)
    edge = REACH * GRID_W
    above = lax.ppermute(kv[tokens - edge :], "sp", [(i, i + 1) for i in range(sp - 1)])
    below = lax.ppermute(kv[:edge], "sp", [(i + 1, i) for i in range(sp - 1)])
    span = 4 if rows % 4 == 0 else 2
    groups = rows // span
    meta = [me_s * rows, sp * rows, 0, 0, -REACH, rows]
    meta += [i * span for i in range(groups)] + list(range(rows))
    q_spec = [(0, 0, tokens)]
    kv_spec = [(0, 0, tokens), (1, 0, edge), (2, 0, edge)]
    attended = attend(
        [q], q_spec, [kv, above, below], kv_spec, ctx, tables, context_bias, meta, span, groups, rows
    )
    full = lax.all_to_all(attended.reshape(tp, own, -1), "tp", split_axis=0, concat_axis=0)
    return out_project(
        [full[i] for i in range(tp)], jnp.arange(tp, dtype=jnp.int32), w_out, resid, mods
    )


CHUNKS = 3


def chunk_row(parity, j, block_rows, chunk_rows):
    return jnp.where(parity == 0, j * chunk_rows, block_rows - (j + 1) * chunk_rows)


def staged_tokens(resid):
    block_rows = resid.shape[0] // GRID_W
    chunk_rows = block_rows // CHUNKS
    parity = lax.axis_index("tp") % 2
    across = []
    for j in range(CHUNKS):
        at = chunk_row(parity, j, block_rows, chunk_rows) * GRID_W
        chunk = lax.dynamic_slice_in_dim(resid, at, chunk_rows * GRID_W)
        across.append(lax.ppermute(chunk, "tp", swap(4, 2)))
    partner = lax.ppermute(resid, "tp", swap(4, 1))
    return partner, across


def staged(resid, mods, staged_in, ctx, tables, weights, gains, context_bias, w_out, heads):
    sp, tp = lax.axis_size("sp"), lax.axis_size("tp")
    me_s, me_t = lax.axis_index("sp"), lax.axis_index("tp")
    parity, chip = me_t % 2, me_t // 2
    own = resid.shape[0]
    block_rows = own // GRID_W
    chunk_rows = block_rows // CHUNKS
    chunk = chunk_rows * GRID_W
    rows = block_rows * tp
    chip_rows = 2 * block_rows
    edge = REACH * GRID_W
    partner, across = staged_in

    def piece_row(source, j):
        return source * block_rows + chunk_row(source % 2, j, block_rows, chunk_rows)

    qs, kvs, q_spec, piece_rows = [], [], [], []

    def project(pieces, piece_at):
        q, kv = qkv(pieces, mods, *weights, *gains, heads)
        at = 0
        for piece, row in zip(pieces, piece_at):
            q_spec.append((len(qs), at, piece.shape[0]))
            piece_rows.append(row)
            at += piece.shape[0]
        qs.append(q)
        kvs.append(kv)

    project([resid, partner], [me_t * block_rows, (me_t ^ 1) * block_rows])
    down = [(s * tp + t, (s - 1) * tp + t) for s in range(1, sp) for t in range(tp)]
    up = [(s * tp + t, (s + 1) * tp + t) for s in range(sp - 1) for t in range(tp)]
    early = [p for p in down if p[0] % tp < 2] + [p for p in up if p[0] % tp >= 2]
    late = [p for p in up if p[0] % tp < 2] + [p for p in down if p[0] % tp >= 2]
    at = jnp.where(chip == parity, 0, own) + jnp.where(chip == 0, 0, own - edge)
    early_kv = lax.ppermute(
        lax.dynamic_slice_in_dim(kvs[0], at, edge), ("sp", "tp"), early
    )
    early_row = jnp.where(chip == 0, rows, -REACH)

    late_kv, late_rows = [], []
    at = jnp.where(chip + parity == 1, 0, chunk)
    beside = lax.ppermute(across[0], "tp", swap(4, 1))
    for j in range(CHUNKS):
        direct, beside = tie((across[j], beside), kvs[-1])
        if j == 0:
            following = lax.ppermute(tie(across[1], kvs[-1]), "tp", swap(4, 1))
        project([direct, beside], [piece_row(me_t ^ 2, j), piece_row(me_t ^ 3, j)])
        beside = following
        if 0 < j < CHUNKS - 1:
            beside = lax.ppermute(tie(across[j + 1], kvs[-1]), "tp", swap(4, 1))
        if j * chunk_rows < REACH:
            late_kv.append(
                lax.ppermute(
                    lax.dynamic_slice_in_dim(kvs[-1], at, chunk), ("sp", "tp"), late
                )
            )
            late_rows.append(
                jnp.where(chip == 0, -(j + 1) * chunk_rows, rows + j * chunk_rows)
            )

    def places(lead):
        return [
            (r + jnp.where(lead == 0, 0, block_rows)) % chip_rows for r in range(chip_rows)
        ]

    span = REACH
    groups = chip_rows // span
    head = [me_s * rows, sp * rows]
    far_groups = [(1 - chip) * chip_rows + i * span for i in range(groups)]
    near_groups = [chip * chip_rows + i * span for i in range(groups)]
    far_spec = [(j - 1, at, size) for j, at, size in q_spec[2:]]
    away = attend(
        qs[1:],
        far_spec,
        kvs + [early_kv],
        q_spec + [(len(kvs), 0, edge)],
        ctx,
        tables,
        context_bias,
        head + piece_rows[2:] + piece_rows + [early_row] + far_groups + places(parity),
        span,
        groups,
        rows,
    )
    from_2 = lax.ppermute(away[:own], "tp", swap(4, 2))
    from_3 = lax.ppermute(away[own:], "tp", swap(4, 3))

    used = 2 + 2 * len(late_kv)
    home = attend(
        [tie(qs[0], away)],
        q_spec[:2],
        kvs[: 1 + len(late_kv)] + late_kv,
        q_spec[:used] + [(1 + len(late_kv) + j, 0, chunk) for j in range(len(late_kv))],
        ctx,
        tables,
        context_bias,
        head + piece_rows[:2] + piece_rows[:used] + late_rows + near_groups + places(parity),
        span,
        groups,
        rows,
    )
    from_1 = lax.ppermute(home[own:], "tp", swap(4, 1))
    spots = me_t ^ jnp.arange(tp, dtype=jnp.int32)
    return out_project([home[:own], from_1, from_2, from_3], spots, w_out, resid, mods)


def shards(
    resid,
    cond,
    mod_shift,
    mod_scale,
    mod_gate,
    norm_gain,
    context,
    w_query,
    w_key,
    w_value,
    query_gain,
    key_gain,
    offset_bias,
    context_bias,
    w_out,
):
    heads = offset_bias.shape[0]
    sp, tp = lax.axis_size("sp"), lax.axis_size("tp")
    me_t = lax.axis_index("tp")
    block_rows = resid.shape[0] // GRID_W
    split = tp == 4 and block_rows % CHUNKS == 0 and 2 * block_rows % REACH == 0
    split = split and REACH % (block_rows // CHUNKS) == 0

    part = mod_part(cond, mod_shift, mod_scale, mod_gate)
    bit = 1
    while bit < sp:
        part = part + lax.ppermute(part, "sp", swap(sp, bit))
        bit *= 2
    if split:
        staged_in = staged_tokens(resid)
    parts = [part]
    bit = tp // 2
    while bit:
        parts += [lax.ppermute(p, "tp", swap(tp, bit)) for p in parts]
        bit //= 2
    spots = [0]
    bit = tp // 2
    while bit:
        spots += [v ^ bit for v in spots]
        bit //= 2
    mods = place_mods(parts, me_t ^ jnp.array(spots, jnp.int32), norm_gain)

    tables = bias_tables(offset_bias)
    ctx = context_kv(context, norm_gain, w_key, w_value, key_gain, heads)
    bit = sp // 2
    while bit:
        ctx = jnp.concatenate([ctx, lax.ppermute(ctx, "sp", swap(sp, bit))], axis=0)
        bit //= 2
    weights, gains = (w_query, w_key, w_value), (query_gain, key_gain)
    if split:
        return staged(
            resid, mods, staged_in, [ctx], tables, weights, gains, context_bias, w_out, heads
        )
    return plain(resid, mods, [ctx], tables, weights, gains, context_bias, w_out, heads)


def solution(mesh):
    in_specs = (
        P(("sp", "tp"), None),
        P("sp"),
        P("sp", "tp"),
        P("sp", "tp"),
        P("sp", "tp"),
        P(),
        P("sp", None),
        P(None, "tp"),
        P(None, "tp"),
        P(None, "tp"),
        P(),
        P(),
        P("tp", None, None),
        P("tp"),
        P(),
    )
    out_specs = P(("sp", "tp"), None)
    return jax.shard_map(shards, mesh=mesh, in_specs=in_specs, out_specs=out_specs, check_vma=False)
```

```python
import functools
import math

import jax
import jax.numpy as jnp
from jax import lax
from jax.experimental import pallas as pl
from jax.experimental.pallas import tpu as pltpu
from jax.sharding import PartitionSpec as P


HEAD_DIM = 128
GRID_W = 64
WIN_ROWS = 8
WIN_COLS = 16
REACH = WIN_ROWS // 2
EPS = 1e-06
LOG2E = math.log2(math.e)
BLANK = 2 * WIN_ROWS
TABLES = BLANK + 1
F32 = jnp.float32
BF16 = jnp.bfloat16
MIB = 1 << 20

VM = pl.BlockSpec(memory_space=pltpu.VMEM)
SM = pl.BlockSpec(memory_space=pltpu.SMEM)


def params(mib):
    return pltpu.CompilerParams(vmem_limit_bytes=mib * MIB)


def cost(flops, nbytes, exps=0):
    return pl.CostEstimate(flops=int(flops), bytes_accessed=int(nbytes), transcendentals=int(exps))


def mod_kernel(cond_ref, shift_ref, scale_ref, gate_ref, out_ref):
    cond = cond_ref[...].astype(F32)
    lifted = cond / (1.0 + jnp.exp(-cond))
    lifted = jnp.broadcast_to(lifted.reshape(1, -1), (16, cond.shape[0])).astype(BF16)
    width = shift_ref.shape[1]
    for i, ref in enumerate((shift_ref, scale_ref, gate_ref)):
        part = jnp.dot(lifted, ref[...], preferred_element_type=F32)
        out_ref[:, i * width : (i + 1) * width] = part[:1]


def mod_part(cond, mod_shift, mod_scale, mod_gate):
    rows, width = mod_shift.shape
    return pl.pallas_call(
        mod_kernel,
        out_shape=jax.ShapeDtypeStruct((1, 3 * width), F32),
        in_specs=[VM] * 4,
        out_specs=VM,
        name="mod_part",
        compiler_params=params(8),
        cost_estimate=cost(96 * rows * width, 6 * rows * width),
    )(cond, mod_shift, mod_scale, mod_gate)


def place_kernel(masks, where_ref, *refs):
    pieces, out_ref = refs[:-1], refs[-1]
    width = pieces[0].shape[1] // 3
    for mask, piece in zip(masks, pieces):
        for j in range(3):
            spot = (where_ref[1] ^ mask) + j * len(masks)
            spot = pl.multiple_of(spot * width, width)
            out_ref[:, pl.ds(spot, width)] = piece[:, j * width : (j + 1) * width]


def small_call(kernel, outs, where, *args):
    return pl.pallas_call(
        kernel,
        out_shape=outs,
        in_specs=[SM] + [VM] * len(args),
        out_specs=jax.tree.map(lambda _: VM, outs),
        compiler_params=params(8),
        cost_estimate=cost(1 << 20, 1 << 16),
    )(where, *args)


def place_mods(pieces, masks, where):
    outs = jax.ShapeDtypeStruct((1, len(pieces) * pieces[0].shape[1]), F32)
    return small_call(functools.partial(place_kernel, masks), outs, where, *pieces)


def add_kernel(where_ref, a_ref, b_ref, out_ref):
    out_ref[...] = a_ref[...] + b_ref[...]


def add(a, b, where):
    return small_call(add_kernel, jax.ShapeDtypeStruct(a.shape, a.dtype), where, a, b)


def join_kernel(where_ref, a_ref, b_ref, out_ref):
    out_ref[: a_ref.shape[0], :] = a_ref[...]
    out_ref[a_ref.shape[0] :, :] = b_ref[...]


def join(a, b, where):
    outs = jax.ShapeDtypeStruct((a.shape[0] + b.shape[0], a.shape[1]), a.dtype)
    return small_call(join_kernel, outs, where, a, b)


def pick_kernel(where_ref, inner_ref, outer_ref, send_ref, keep_ref):
    mine = (where_ref[1] & 1) + (where_ref[1] >> 1) == 1

    @pl.when(mine)
    def _():
        send_ref[...] = outer_ref[...]
        keep_ref[...] = inner_ref[...]

    @pl.when(~mine)
    def _():
        send_ref[...] = inner_ref[...]
        keep_ref[...] = outer_ref[...]


def pick(inner, outer, where):
    outs = jax.ShapeDtypeStruct(inner.shape, inner.dtype)
    return small_call(pick_kernel, (outs, outs), where, inner, outer)


def cut_kernel(where_ref, x_ref, *outs):
    count = x_ref.shape[0]
    size = outs[0].shape[0]
    for j, out_ref in enumerate(outs):
        at = jnp.where((where_ref[1] & 1) == 0, j * size, count - (j + 1) * size)
        out_ref[...] = x_ref[pl.ds(pl.multiple_of(at, GRID_W), size), :]


def cut_chunks(x, count, where):
    outs = jax.ShapeDtypeStruct((x.shape[0] // count, x.shape[1]), x.dtype)
    return small_call(cut_kernel, (outs,) * count, where, x)


def table_kernel(bias_ref, out_ref):
    heads = out_ref.shape[0]
    column = lax.broadcasted_iota(jnp.int32, (GRID_W, 2 * GRID_W), 0)
    lane = lax.broadcasted_iota(jnp.int32, (GRID_W, 2 * GRID_W), 1)
    left = lane < GRID_W
    begin = jnp.clip(column - WIN_COLS // 2, 0, GRID_W - WIN_COLS)
    key = jnp.where(left, lane, lane - GRID_W)
    valid = (key >= begin) & (key < begin + WIN_COLS)
    empty = jnp.full((GRID_W, 2 * GRID_W), -1e30, F32)
    for h in range(heads):
        rolled = []
        for d in range(2 * WIN_ROWS - 1):
            row = jnp.broadcast_to(bias_ref[h, d : d + 1, :] * LOG2E, (GRID_W, 2 * GRID_W))
            lo = pltpu.roll(row, 2 * GRID_W - WIN_COLS + 1, 1, stride=1, stride_axis=0)
            hi = pltpu.roll(row, GRID_W - WIN_COLS + 1, 1, stride=1, stride_axis=0)
            rolled.append((jnp.where(valid & left, lo, empty), jnp.where(valid & ~left, hi, empty)))
        for d in range(2 * WIN_ROWS - 2):
            out_ref[h, d] = jnp.where(left, rolled[d][0], rolled[d + 1][1])
        out_ref[h, 2 * WIN_ROWS - 2] = rolled[WIN_ROWS + 2][0]
        out_ref[h, 2 * WIN_ROWS - 1] = rolled[WIN_ROWS - REACH - 1][1]
        out_ref[h, BLANK] = empty


def bias_tables(offset_bias):
    heads, rows, cols = offset_bias.shape
    padded = jnp.pad(offset_bias, ((0, 0), (0, 16 - rows), (0, 2 * GRID_W - cols)))
    return pl.pallas_call(
        table_kernel,
        out_shape=jax.ShapeDtypeStruct((heads, TABLES, GRID_W, 2 * GRID_W), F32),
        in_specs=[VM],
        out_specs=VM,
        name="bias_tables",
        compiler_params=params(8),
        cost_estimate=cost(1 << 22, heads * TABLES * GRID_W * 2 * GRID_W * 4),
    )(padded)


def normed_heads(values, gain, heads):
    parts = []
    for h in range(heads):
        part = values[:, h * HEAD_DIM : (h + 1) * HEAD_DIM]
        square = jnp.mean(part * part, axis=-1, keepdims=True)
        parts.append((part * lax.rsqrt(square + EPS) * gain).astype(BF16))
    return jnp.concatenate(parts, axis=1)


def qkv_kernel(count, heads, tile, take, carried, *refs):
    where_ref, pieces = refs[0], refs[1 : 1 + count]
    refs = refs[1 + count :]
    had, refs = refs[:carried], refs[carried:]
    ma_ref, mb_ref, ng_ref, wq_ref, wk_ref, wv_ref, qg_ref, kg_ref, q_ref, kv_ref = refs[:10]
    edge_ref = refs[10] if take else None
    raw, normed, affine = refs[-3:]
    width = heads * HEAD_DIM
    depth = ng_ref.shape[1]
    strip = 16
    affine[0:1, :] = ma_ref[:, :depth] + mb_ref[:, :depth]
    affine[1:2, :] = ng_ref[...] * (1.0 + (ma_ref[:, depth : 2 * depth] + mb_ref[:, depth : 2 * depth]))
    base = 0
    for piece in pieces:
        raw[base : base + piece.shape[0], :] = piece[...]
        base += piece.shape[0]
    tiles = base // tile
    step = min(width, 2 * HEAD_DIM)
    steps = [(w, at) for w in range(3) for at in range(0, width, step)]
    strips = tile // strip

    def norm_strip(source, slot, j):
        floats = raw[pl.ds(pl.multiple_of(source + j * strip, strip), strip), :].astype(F32)
        inverse = lax.rsqrt(jnp.mean(floats * floats, axis=-1, keepdims=True) + EPS)
        normed[slot, j * strip : (j + 1) * strip, :] = (
            floats * inverse * affine[1:2, :] + affine[0:1, :]
        ).astype(BF16)

    for j in range(strips):
        norm_strip(0, 0, j)

    def store(rows, w, at, values):
        cols = slice(at, at + step)
        if w == 0:
            q_ref[rows, cols] = normed_heads(values, qg_ref[...], step // HEAD_DIM)
        elif w == 1:
            kv_ref[rows, cols] = normed_heads(values, kg_ref[...], step // HEAD_DIM)
        else:
            kv_ref[rows, width + at : width + at + step] = values.astype(BF16)

    def project(i, _, last=False):
        slot = lax.rem(i, 2)
        rows = pl.ds(pl.multiple_of(i * tile, tile), tile)
        held = None
        done = 0
        for n, (w, at) in enumerate(steps):
            ref = (wq_ref, wk_ref, wv_ref)[w]
            values = jnp.dot(
                normed[slot], ref[:, at : at + step], preferred_element_type=F32
            )
            if held is not None:
                store(rows, *held)
            upto = strips * (n + 1) // len(steps)
            while done < upto and not last:
                norm_strip((i + 1) * tile, 1 - slot, done)
                done += 1
            held = (w, at, values)
        store(rows, *held)
        return 0

    lax.fori_loop(0, tiles - 1, project, 0)
    project(tiles - 1, 0, True)
    if take:
        at = 0
        for ref in had:
            edge_ref[: ref.shape[0], :] = ref[...]
            at = ref.shape[0]
        size = edge_ref.shape[0] - at
        start = pl.multiple_of(take(where_ref[0], where_ref[1]), GRID_W)
        edge_ref[at:, :] = kv_ref[pl.ds(start, size), :]


def qkv(
    where,
    pieces,
    mods,
    norm_gain,
    w_query,
    w_key,
    w_value,
    query_gain,
    key_gain,
    heads,
    take=None,
    taken=0,
    had=(),
):
    total = sum(p.shape[0] for p in pieces)
    depth, width = w_query.shape
    tile = 256 if total % 256 == 0 else 128
    outs = [
        jax.ShapeDtypeStruct((total, width), BF16),
        jax.ShapeDtypeStruct((total, 2 * width), BF16),
    ]
    if take:
        outs.append(jax.ShapeDtypeStruct((taken, 2 * width), BF16))
    return pl.pallas_call(
        functools.partial(qkv_kernel, len(pieces), heads, tile, take, len(had)),
        out_shape=tuple(outs),
        in_specs=[SM] + [VM] * (len(pieces) + len(had) + 8),
        out_specs=tuple(VM for _ in outs),
        scratch_shapes=[
            pltpu.VMEM((total, depth), BF16),
            pltpu.VMEM((2, tile, depth), BF16),
            pltpu.VMEM((2, depth), F32),
        ],
        name="qkv",
        compiler_params=params(24),
        cost_estimate=cost(6 * total * depth * width, total * depth * 2 + 6 * depth * width),
    )(
        where,
        *pieces,
        *had,
        *mods,
        norm_gain.reshape(1, -1),
        w_query,
        w_key,
        w_value,
        query_gain.reshape(1, -1),
        key_gain.reshape(1, -1),
    )


def context_kernel(heads, x_ref, gain_ref, wk_ref, wv_ref, kg_ref, kv_ref):
    width = heads * HEAD_DIM
    floats = x_ref[...].astype(F32)
    inverse = lax.rsqrt(jnp.mean(floats * floats, axis=-1, keepdims=True) + EPS)
    x = (floats * inverse * gain_ref[...]).astype(BF16)
    kv_ref[:, :width] = normed_heads(
        jnp.dot(x, wk_ref[...], preferred_element_type=F32), kg_ref[...], heads
    )
    kv_ref[:, width:] = jnp.dot(x, wv_ref[...], preferred_element_type=F32).astype(BF16)


def context_kv(context, norm_gain, w_key, w_value, key_gain, heads):
    count, depth = context.shape
    width = w_key.shape[1]
    return pl.pallas_call(
        functools.partial(context_kernel, heads),
        out_shape=jax.ShapeDtypeStruct((count, 2 * width), BF16),
        in_specs=[VM] * 5,
        out_specs=VM,
        name="context_kv",
        compiler_params=params(16),
        cost_estimate=cost(4 * count * depth * width, 4 * depth * width),
    )(context, norm_gain.reshape(1, -1), w_key, w_value, key_gain.reshape(1, -1))


def attend_kernel(
    heads, span, groups, q_spec, kv_spec, n_ctx, rows_of, total, where_ref, cbias_ref, *refs
):
    n_q, n_kv = q_spec[-1][0] + 1, kv_spec[-1][0] + 1
    q_refs, refs = refs[:n_q], refs[n_q:]
    kv_refs, refs = refs[:n_kv], refs[n_kv:]
    ctx_refs, refs = refs[:n_ctx], refs[n_ctx:]
    tab_ref, out_ref, keys, queries, context, scores, weights = refs
    width = heads * HEAD_DIM
    block = span * GRID_W
    key_rows = span + WIN_ROWS
    window = key_rows * GRID_W
    ctx_count = context.shape[0]
    factor = LOG2E * HEAD_DIM**-0.5
    lines = 2 * GRID_W
    first, rows_at = rows_of(where_ref[0], where_ref[1])
    base = 0
    for i, (j, at, size) in enumerate(q_spec):
        to = pl.multiple_of(rows_at[base + i] * GRID_W, GRID_W)
        queries[pl.ds(to, size), :] = q_refs[j][at : at + size, :]
    base += len(q_spec)
    for i, (j, at, size) in enumerate(kv_spec):
        to = pl.multiple_of((rows_at[base + i] + REACH) * GRID_W, GRID_W)
        keys[pl.ds(to, size), :] = kv_refs[j][at : at + size, :]
    base += len(kv_spec)
    at = 0
    for ref in ctx_refs:
        context[at : at + ref.shape[0], :] = ref[...]
        at += ref.shape[0]
    nt = (((1,), (1,)), ((), ()))

    def group(i, _):
        row = rows_at[base] + i * span
        q_at = pl.multiple_of(row * GRID_W, GRID_W)
        top = first + row
        start = jnp.clip(top - REACH, 0, total - key_rows)
        k_at = pl.multiple_of((start - first + REACH) * GRID_W, GRID_W)
        spots = []
        for r in range(span):
            g = top + r
            a = jnp.clip(g - REACH, 0, total - WIN_ROWS)
            for p in range(key_rows // 2):
                u = start + 2 * p
                lv = (u >= a) & (u < a + WIN_ROWS)
                rv = (u + 1 >= a) & (u + 1 < a + WIN_ROWS)
                both = jnp.where(rv, u - g + WIN_ROWS - 1, BLANK - 2)
                spots.append(jnp.where(lv, both, jnp.where(rv, BLANK - 1, BLANK)))

        def score(h):
            hk = slice(h * HEAD_DIM, (h + 1) * HEAD_DIM)
            q = queries[pl.ds(q_at, block), hk]
            scores[h % 2, :, :window] = lax.dot_general(
                q, keys[pl.ds(k_at, window), hk], nt, preferred_element_type=F32
            )
            scores[h % 2, :, window:] = lax.dot_general(
                q, context[:, hk], nt, preferred_element_type=F32
            )

        def soften(h):
            cbias = cbias_ref[h] * LOG2E
            sums = []
            for r in range(span):
                rows = slice(r * GRID_W, (r + 1) * GRID_W)
                tops = None
                for p in range(key_rows // 2):
                    cols = slice(p * lines, (p + 1) * lines)
                    tile = scores[h % 2, rows, cols] * factor
                    tile = tile + tab_ref[h, spots[r * (key_rows // 2) + p]]
                    scores[h % 2, rows, cols] = tile
                    tops = tile if tops is None else jnp.maximum(tops, tile)
                ctx = scores[h % 2, rows, window : window + lines]
                for p in range(1, ctx_count // lines):
                    cols = slice(window + p * lines, window + (p + 1) * lines)
                    ctx = jnp.maximum(ctx, scores[h % 2, rows, cols])
                tops = jnp.maximum(tops, ctx * factor + cbias)
                high = jnp.max(tops, axis=1, keepdims=True)
                acc = None
                for p in range(key_rows // 2 + ctx_count // lines):
                    cols = slice(p * lines, (p + 1) * lines)
                    tile = scores[h % 2, rows, cols]
                    if p < key_rows // 2:
                        tile = jnp.exp2(tile - high)
                    else:
                        tile = jnp.exp2(tile * factor - (high - cbias))
                    acc = tile if acc is None else acc + tile
                    weights[h % 2, rows, cols] = tile.astype(BF16)
                sums.append(jnp.sum(acc, axis=1, keepdims=True))
            return sums

        def combine(h, sums):
            hk = slice(h * HEAD_DIM, (h + 1) * HEAD_DIM)
            hv = slice(width + h * HEAD_DIM, width + (h + 1) * HEAD_DIM)
            out = jnp.dot(
                weights[h % 2, :, :window], keys[pl.ds(k_at, window), hv], preferred_element_type=F32
            )
            out = out + jnp.dot(
                weights[h % 2, :, window:], context[:, hv], preferred_element_type=F32
            )
            out = (out / jnp.concatenate(sums, axis=0)).astype(BF16)
            out_ref[pl.ds(i * block if groups == 1 else pl.multiple_of(i * block, block), block), hk] = out

        score(0)
        held = None
        for h in range(heads):
            if h + 1 < heads:
                score(h + 1)
            sums = soften(h)
            if held is not None:
                combine(*held)
            held = (h, sums)
        combine(*held)
        return 0

    if groups == 1:
        group(0, 0)
    else:
        lax.fori_loop(0, groups, group, 0)


def attend(
    where, queries, q_spec, kvs, kv_spec, ctx, tables, context_bias, rows_of, total, span, groups, rows
):
    heads = tables.shape[0]
    width = heads * HEAD_DIM
    block = span * GRID_W
    ctx_count = sum(c.shape[0] for c in ctx)
    keys = (span + WIN_ROWS) * GRID_W + ctx_count
    elements = groups * block * heads * keys
    return pl.pallas_call(
        functools.partial(
            attend_kernel, heads, span, groups, q_spec, kv_spec, len(ctx), rows_of, total
        ),
        out_shape=jax.ShapeDtypeStruct((groups * block, width), BF16),
        in_specs=[SM, SM] + [VM] * (len(queries) + len(kvs) + len(ctx) + 1),
        out_specs=VM,
        scratch_shapes=[
            pltpu.VMEM(((rows + 2 * REACH) * GRID_W, 2 * width), BF16),
            pltpu.VMEM((rows * GRID_W, width), BF16),
            pltpu.VMEM((ctx_count, 2 * width), BF16),
            pltpu.VMEM((2, block, keys), F32),
            pltpu.VMEM((2, block, keys), BF16),
        ],
        name="attend",
        compiler_params=params(28),
        cost_estimate=cost(8 * elements * HEAD_DIM, 8 << 20, elements),
    )(where, context_bias, *queries, *kvs, *ctx, tables)


def out_kernel(masks, tile, final, where_ref, *refs):
    count = len(masks)
    pieces, refs = refs[:count], refs[count:]
    w_ref = refs[0]
    before = refs[1:-1]
    out_ref = refs[-1]
    depth = pieces[0].shape[1]
    width = w_ref.shape[1]

    def one(i, _):
        cols = pl.ds(pl.multiple_of(i * tile, tile), tile)
        total = None
        for j, piece in enumerate(pieces):
            rows = pl.ds(pl.multiple_of(masks[j](where_ref[1]) * depth, depth), depth)
            part = jnp.dot(piece[...], w_ref[rows, cols], preferred_element_type=F32)
            total = part if total is None else total + part
        if final:
            resid_ref, ma_ref, mb_ref = before[:3]
            for ref in before[3:]:
                total = total + ref[:, cols]
            spot = pl.ds(pl.multiple_of(2 * width + i * tile, tile), tile)
            gate = ma_ref[:, spot] + mb_ref[:, spot]
            out_ref[:, cols] = (resid_ref[:, cols].astype(F32) + gate * total).astype(BF16)
        else:
            out_ref[:, cols] = total
        return 0

    lax.fori_loop(0, width // tile, one, 0, unroll=2)


def out_project(where, pieces, masks, w_out, before=(), final=True):
    count, width = pieces[0].shape[0], w_out.shape[1]
    depth = sum(p.shape[1] for p in pieces)
    return pl.pallas_call(
        functools.partial(out_kernel, masks, 256, final),
        out_shape=jax.ShapeDtypeStruct((count, width), BF16 if final else F32),
        in_specs=[SM] + [VM] * (len(pieces) + 1 + len(before)),
        out_specs=VM,
        name="out_project",
        compiler_params=params(16),
        cost_estimate=cost(2 * count * width * depth, 2 * depth * width + 8 * count * width),
    )(where, *pieces, w_out, *before)


def swap(count, bit):
    return [(i, i ^ bit) for i in range(count)]


def tie(value, other):
    return lax.optimization_barrier((value, other))[0]


def plain(where, resid, mods, norm_gain, ctx, tables, weights, gains, context_bias, w_out, heads):
    sp, tp = lax.axis_size("sp"), lax.axis_size("tp")
    own = resid.shape[0]
    tokens = own * tp
    rows = tokens // GRID_W
    piece = lax.all_gather(resid, "tp", axis=0, tiled=True)
    q, kv = qkv(where, [piece], mods, norm_gain, *weights, *gains, heads)
    edge = REACH * GRID_W
    above = lax.ppermute(kv[tokens - edge :], "sp", [(i, i + 1) for i in range(sp - 1)])
    below = lax.ppermute(kv[:edge], "sp", [(i + 1, i) for i in range(sp - 1)])
    span = 4 if rows % 4 == 0 else 2
    attended = attend(
        where,
        [q],
        [(0, 0, tokens)],
        [kv, above, below],
        [(0, 0, tokens), (1, 0, edge), (2, 0, edge)],
        ctx,
        tables,
        context_bias,
        lambda s, t: (s * rows, [0, 0, -REACH, rows, 0]),
        sp * rows,
        span,
        rows // span,
        rows,
    )
    full = lax.all_to_all(attended.reshape(tp, own, -1), "tp", split_axis=0, concat_axis=0)
    masks = [lambda t, i=i: jnp.int32(i) for i in range(tp)]
    return out_project(where, [full[i] for i in range(tp)], masks, w_out, (resid, *mods))


CHUNKS = 3


def chunk_row(source, j, block_rows, chunk_rows):
    return source * block_rows + jnp.where(
        (source & 1) == 0, j * chunk_rows, block_rows - (j + 1) * chunk_rows
    )


def staged_tokens(where, resid):
    across = []
    for chunk in cut_chunks(resid, CHUNKS, where):
        across.append(lax.ppermute(chunk, "tp", swap(4, 2)))
    partner = lax.ppermute(resid, "tp", swap(4, 1))
    return partner, across


def staged(
    where, resid, mods, norm_gain, staged_in, ctx, tables, weights, gains, context_bias, w_out, heads
):
    sp, tp = lax.axis_size("sp"), lax.axis_size("tp")
    own = resid.shape[0]
    block_rows = own // GRID_W
    chunk_rows = block_rows // CHUNKS
    chunk = chunk_rows * GRID_W
    rows = block_rows * tp
    edge = REACH * GRID_W
    partner, across = staged_in
    project = functools.partial(
        qkv,
        where,
        mods=mods,
        norm_gain=norm_gain,
        w_query=weights[0],
        w_key=weights[1],
        w_value=weights[2],
        query_gain=gains[0],
        key_gain=gains[1],
        heads=heads,
    )

    def near_rows(t):
        return [t * block_rows, (t ^ 1) * block_rows]

    def chunk_rows_of(t, j):
        return [chunk_row(t ^ mask, j, block_rows, chunk_rows) for mask in (2, 3)]

    def early_at(s, t):
        chip, parity = t >> 1, t & 1
        return jnp.where(chip == parity, 0, own) + jnp.where(chip == 0, 0, own - edge)

    def late_at(s, t):
        return jnp.where((t >> 1) + (t & 1) == 1, 0, chunk)

    down = [(s * tp + t, (s - 1) * tp + t) for s in range(1, sp) for t in range(tp)]
    up = [(s * tp + t, (s + 1) * tp + t) for s in range(sp - 1) for t in range(tp)]
    early = [p for p in down if p[0] % tp < 2] + [p for p in up if p[0] % tp >= 2]
    late = [p for p in up if p[0] % tp < 2] + [p for p in down if p[0] % tp >= 2]

    q0, kv0, edge_kv = project([resid, partner], take=early_at, taken=edge)
    early_kv = lax.ppermute(edge_kv, ("sp", "tp"), early)
    beside0 = lax.ppermute(across[0], "tp", swap(4, 1))
    beside1 = lax.ppermute(tie(across[1], kv0), "tp", swap(4, 1))
    q1, kv1, edge_kv = project(list(tie((across[0], beside0), kv0)), take=late_at, taken=chunk)
    q2, kv2, edge_kv = project(
        list(tie((across[1], beside1), kv1)), take=late_at, taken=2 * chunk, had=(edge_kv,)
    )
    late_kv = lax.ppermute(edge_kv, ("sp", "tp"), late)

    near = [(0, 0, own), (0, own, own)]
    pair = [(0, chunk), (chunk, chunk)]
    kv_spec = near + [(j, at, size) for j in (1, 2, 3) for at, size in pair]

    def block(queries, q_spec, kvs, kv_spec, rows_of):
        return attend(
            where,
            queries,
            q_spec,
            kvs,
            kv_spec,
            ctx,
            tables,
            context_bias,
            rows_of,
            sp * rows,
            block_rows,
            1,
            rows,
        )

    def home_rows(last, late):
        def rows_of(s, t):
            chip = t >> 1
            at = near_rows(t) + near_rows(t) + chunk_rows_of(t, 0) + chunk_rows_of(t, 1)
            if late:
                for j in range(2):
                    at.append(jnp.where(chip == 0, -(j + 1) * chunk_rows, rows + j * chunk_rows))
            return s * rows, at + [last(chip) * block_rows]

        return rows_of

    inner = block([q0], near, [kv0, kv1, kv2], kv_spec[:6], home_rows(lambda chip: 1 + chip, False))

    beside2 = lax.ppermute(tie(across[2], inner), "tp", swap(4, 1))
    q3, kv3 = project(list(tie((across[2], beside2), inner)))

    def far(mask, after):
        def rows_of(s, t):
            chunks = [row for j in range(CHUNKS) for row in chunk_rows_of(t, j)]
            outside = jnp.where(t < 2, rows, -REACH)
            return s * rows, chunks + near_rows(t) + chunks + [outside, (t ^ mask) * block_rows]

        return block(
            [tie(q1, after), q2, q3],
            [(j - 1, at, size) for j, at, size in kv_spec[2:]],
            [kv0, kv1, kv2, kv3, early_kv],
            kv_spec + [(4, 0, edge)],
            rows_of,
        )

    away2 = far(2, kv3)
    from_2 = lax.ppermute(away2, "tp", swap(4, 2))
    away3 = far(3, away2)
    from_3 = lax.ppermute(away3, "tp", swap(4, 3))

    outer = block(
        [tie(q0, away3)],
        near,
        [kv0, kv1, kv2, late_kv],
        kv_spec[:6] + [(3, at, size) for at, size in pair],
        home_rows(lambda chip: 3 * chip, True),
    )
    send, keep = pick(inner, outer, where)
    from_1 = lax.ppermute(send, "tp", swap(4, 1))
    masks = [lambda t, i=i: t ^ i for i in range(4)]
    partial = out_project(where, [keep, from_1, from_2], masks[:3], w_out, final=False)
    return out_project(where, [from_3], masks[3:], w_out, (resid, *mods, partial))


def shards(
    resid,
    cond,
    mod_shift,
    mod_scale,
    mod_gate,
    norm_gain,
    context,
    w_query,
    w_key,
    w_value,
    query_gain,
    key_gain,
    offset_bias,
    context_bias,
    w_out,
):
    heads = offset_bias.shape[0]
    sp, tp = lax.axis_size("sp"), lax.axis_size("tp")
    block_rows = resid.shape[0] // GRID_W
    split = tp == 4 and sp > 1 and block_rows == CHUNKS * REACH // 2
    where = jnp.stack([lax.axis_index("sp"), lax.axis_index("tp")]).astype(jnp.int32)

    tables = bias_tables(offset_bias)
    parts = [mod_part(cond, mod_shift, mod_scale, mod_gate)]
    masks = [0]
    bit = tp // 2
    while bit:
        parts += [lax.ppermute(p, "tp", swap(tp, bit)) for p in parts]
        masks += [v ^ bit for v in masks]
        bit //= 2
    run = plain
    if split:
        run = functools.partial(staged, staged_in=staged_tokens(where, resid))
    mods = place_mods(tie(parts, tables), masks, where)
    bit = 1
    while bit < sp:
        other = lax.ppermute(mods, "sp", swap(sp, bit))
        bit *= 2
        if bit < sp:
            mods = add(mods, other, where)

    ctx = context_kv(context, norm_gain, w_key, w_value, key_gain, heads)
    bit = sp // 2
    while bit:
        got = lax.ppermute(ctx, "sp", swap(sp, bit))
        bit //= 2
        if bit:
            ctx = join(ctx, got, where)
    return run(
        where,
        resid,
        (mods, other),
        norm_gain,
        ctx=[ctx, got],
        tables=tables,
        weights=(w_query, w_key, w_value),
        gains=(query_gain, key_gain),
        context_bias=context_bias,
        w_out=w_out,
        heads=heads,
    )


def solution(mesh):
    in_specs = (
        P(("sp", "tp"), None),
        P("sp"),
        P("sp", "tp"),
        P("sp", "tp"),
        P("sp", "tp"),
        P(),
        P("sp", None),
        P(None, "tp"),
        P(None, "tp"),
        P(None, "tp"),
        P(),
        P(),
        P("tp", None, None),
        P("tp"),
        P(),
    )
    out_specs = P(("sp", "tp"), None)
    return jax.shard_map(shards, mesh=mesh, in_specs=in_specs, out_specs=out_specs, check_vma=False)
```

```python
import functools
import math

import jax
import jax.numpy as jnp
from jax import lax
from jax.experimental import pallas as pl
from jax.experimental.pallas import tpu as pltpu
from jax.sharding import PartitionSpec as P


HEAD_DIM = 128
GRID_W = 64
WIN_ROWS = 8
WIN_COLS = 16
REACH = WIN_ROWS // 2
LUMP = 16
EPS = 1e-06
LOG2E = math.log2(math.e)
BLANK = 2 * WIN_ROWS
TABLES = BLANK + 1
F32 = jnp.float32
BF16 = jnp.bfloat16
MIB = 1 << 20

VM = pl.BlockSpec(memory_space=pltpu.VMEM)
SM = pl.BlockSpec(memory_space=pltpu.SMEM)


def params(mib):
    return pltpu.CompilerParams(vmem_limit_bytes=mib * MIB)


def cost(flops, nbytes, exps=0):
    return pl.CostEstimate(flops=int(flops), bytes_accessed=int(nbytes), transcendentals=int(exps))


HBM = pl.BlockSpec(memory_space=pltpu.HBM)


def mod_kernel(cond_hbm, *refs):
    maps, part_ref, cond_ref, held, sems = refs[:3], *refs[3:]
    copies = [pltpu.make_async_copy(cond_hbm, cond_ref, sems.at[0])]
    for i, ref in enumerate(maps):
        copies.append(pltpu.make_async_copy(ref, held.at[i], sems.at[1 + i]))
    for copy in copies:
        copy.start()
    copies[0].wait()
    cond = cond_ref[...].astype(F32)
    lifted = cond / (1.0 + jnp.exp(-cond))
    lifted = jnp.broadcast_to(lifted.reshape(1, -1), (16, cond.shape[0])).astype(BF16)
    width = held.shape[2]
    for i in range(3):
        copies[1 + i].wait()
        part = jnp.dot(lifted, held[i], preferred_element_type=F32)
        part_ref[:, i * width : (i + 1) * width] = part[:1]


def mod_part(cond, mod_shift, mod_scale, mod_gate):
    rows, width = mod_shift.shape
    return pl.pallas_call(
        mod_kernel,
        out_shape=jax.ShapeDtypeStruct((1, 3 * width), F32),
        in_specs=[HBM] * 4,
        out_specs=VM,
        scratch_shapes=[
            pltpu.VMEM((rows,), BF16),
            pltpu.VMEM((3, rows, width), BF16),
            pltpu.SemaphoreType.DMA((4,)),
        ],
        name="mod_part",
        compiler_params=params(60),
        cost_estimate=cost(96 * rows * width, 6 * rows * width),
    )(cond, mod_shift, mod_scale, mod_gate)


def cut_kernel(where_ref, x_ref, *refs):
    outs, sems = refs[:-1], refs[-1]
    copies = []
    for j, out_ref in enumerate(outs):
        size = out_ref.shape[0]
        at = jnp.where((where_ref[1] & 1) == 0, j * size, x_ref.shape[0] - (j + 1) * size)
        at = pl.multiple_of(at, GRID_W)
        copies.append(pltpu.make_async_copy(x_ref.at[pl.ds(at, size), :], out_ref, sems.at[j]))
    for copy in copies:
        copy.start()
    for copy in copies:
        copy.wait()


def cut_chunks(where, x, count):
    outs = (jax.ShapeDtypeStruct((x.shape[0] // count, x.shape[1]), x.dtype),) * count
    return pl.pallas_call(
        cut_kernel,
        out_shape=outs,
        in_specs=[SM, HBM],
        out_specs=(VM,) * count,
        scratch_shapes=[pltpu.SemaphoreType.DMA((count,))],
        name="cut",
        compiler_params=params(8),
        cost_estimate=cost(1 << 20, 4 * x.size),
    )(where, x)


def place_kernel(masks, where_ref, *refs):
    pieces, out_ref = refs[:-1], refs[-1]
    width = pieces[0].shape[1] // 3
    for mask, piece in zip(masks, pieces):
        for j in range(3):
            spot = (where_ref[1] ^ mask) + j * len(masks)
            spot = pl.multiple_of(spot * width, width)
            out_ref[:, pl.ds(spot, width)] = piece[:, j * width : (j + 1) * width]


def small_call(kernel, outs, where, *args):
    return pl.pallas_call(
        kernel,
        out_shape=outs,
        in_specs=[SM] + [VM] * len(args),
        out_specs=jax.tree.map(lambda _: VM, outs),
        compiler_params=params(8),
        cost_estimate=cost(1 << 20, 1 << 16),
    )(where, *args)


def place_mods(pieces, masks, where):
    outs = jax.ShapeDtypeStruct((1, len(pieces) * pieces[0].shape[1]), F32)
    return small_call(functools.partial(place_kernel, masks), outs, where, *pieces)


def add_kernel(where_ref, a_ref, b_ref, out_ref):
    out_ref[...] = a_ref[...] + b_ref[...]


def add(a, b, where):
    return small_call(add_kernel, jax.ShapeDtypeStruct(a.shape, a.dtype), where, a, b)


def join_kernel(where_ref, a_ref, b_ref, out_ref):
    out_ref[: a_ref.shape[0], :] = a_ref[...]
    out_ref[a_ref.shape[0] :, :] = b_ref[...]


def join(a, b, where):
    outs = jax.ShapeDtypeStruct((a.shape[0] + b.shape[0], a.shape[1]), a.dtype)
    return small_call(join_kernel, outs, where, a, b)


def pick_kernel(where_ref, inner_ref, outer_ref, send_ref, keep_ref):
    mine = (where_ref[1] & 1) + (where_ref[1] >> 1) == 1

    @pl.when(mine)
    def _():
        send_ref[...] = outer_ref[...]
        keep_ref[...] = inner_ref[...]

    @pl.when(~mine)
    def _():
        send_ref[...] = inner_ref[...]
        keep_ref[...] = outer_ref[...]


def pick(inner, outer, where):
    outs = jax.ShapeDtypeStruct(inner.shape, inner.dtype)
    return small_call(pick_kernel, (outs, outs), where, inner, outer)


def table_kernel(bias_ref, out_ref):
    heads = out_ref.shape[0]
    column = lax.broadcasted_iota(jnp.int32, (GRID_W, 2 * GRID_W), 0)
    lane = lax.broadcasted_iota(jnp.int32, (GRID_W, 2 * GRID_W), 1)
    left = lane < GRID_W
    begin = jnp.clip(column - WIN_COLS // 2, 0, GRID_W - WIN_COLS)
    key = jnp.where(left, lane, lane - GRID_W)
    valid = (key >= begin) & (key < begin + WIN_COLS)
    empty = jnp.full((GRID_W, 2 * GRID_W), -1e30, F32)
    for h in range(heads):
        rolled = []
        for d in range(2 * WIN_ROWS - 1):
            row = jnp.broadcast_to(bias_ref[h, d : d + 1, :] * LOG2E, (GRID_W, 2 * GRID_W))
            lo = pltpu.roll(row, 2 * GRID_W - WIN_COLS + 1, 1, stride=1, stride_axis=0)
            hi = pltpu.roll(row, GRID_W - WIN_COLS + 1, 1, stride=1, stride_axis=0)
            rolled.append((jnp.where(valid & left, lo, empty), jnp.where(valid & ~left, hi, empty)))
        for d in range(2 * WIN_ROWS - 2):
            out_ref[h, d] = jnp.where(left, rolled[d][0], rolled[d + 1][1])
        out_ref[h, 2 * WIN_ROWS - 2] = rolled[WIN_ROWS + 2][0]
        out_ref[h, 2 * WIN_ROWS - 1] = rolled[WIN_ROWS - REACH - 1][1]
        out_ref[h, BLANK] = empty


def bias_tables(offset_bias):
    heads, rows, cols = offset_bias.shape
    padded = jnp.pad(offset_bias, ((0, 0), (0, 16 - rows), (0, 2 * GRID_W - cols)))
    return pl.pallas_call(
        table_kernel,
        out_shape=jax.ShapeDtypeStruct((heads, TABLES, GRID_W, 2 * GRID_W), F32),
        in_specs=[VM],
        out_specs=VM,
        name="bias_tables",
        compiler_params=params(8),
        cost_estimate=cost(1 << 22, heads * TABLES * GRID_W * 2 * GRID_W * 4),
    )(padded)


def normed_heads(values, gain, heads):
    parts = []
    for h in range(heads):
        part = values[:, h * HEAD_DIM : (h + 1) * HEAD_DIM]
        square = jnp.mean(part * part, axis=-1, keepdims=True)
        parts.append((part * lax.rsqrt(square + EPS) * gain).astype(BF16))
    return jnp.concatenate(parts, axis=1)


def qkv_kernel(count, heads, tile, take, *refs):
    where_ref, pieces = refs[0], refs[1 : 1 + count]
    refs = refs[1 + count :]
    ma_ref, mb_ref, ng_ref, wq_ref, wk_ref, wv_ref, qg_ref, kg_ref, q_ref, kv_ref = refs[:10]
    edge_ref = refs[10] if take else None
    raw, normed, affine = refs[-3:]
    width = heads * HEAD_DIM
    depth = ng_ref.shape[1]
    strip = 16
    affine[0:1, :] = ma_ref[:, :depth] + mb_ref[:, :depth]
    affine[1:2, :] = ng_ref[...] * (1.0 + (ma_ref[:, depth : 2 * depth] + mb_ref[:, depth : 2 * depth]))
    base = 0
    for piece in pieces:
        raw[base : base + piece.shape[0], :] = piece[...]
        base += piece.shape[0]
    tiles = base // tile
    step = min(width, 2 * HEAD_DIM)
    steps = [(w, at) for w in range(3) for at in range(0, width, step)]
    strips = tile // strip

    def norm_strip(source, slot, j):
        floats = raw[pl.ds(pl.multiple_of(source + j * strip, strip), strip), :].astype(F32)
        inverse = lax.rsqrt(jnp.mean(floats * floats, axis=-1, keepdims=True) + EPS)
        normed[slot, j * strip : (j + 1) * strip, :] = (
            floats * inverse * affine[1:2, :] + affine[0:1, :]
        ).astype(BF16)

    for j in range(strips):
        norm_strip(0, 0, j)

    def store(rows, w, at, values):
        cols = slice(at, at + step)
        if w == 0:
            q_ref[rows, cols] = normed_heads(values, qg_ref[...], step // HEAD_DIM)
        elif w == 1:
            kv_ref[rows, cols] = normed_heads(values, kg_ref[...], step // HEAD_DIM)
        else:
            kv_ref[rows, width + at : width + at + step] = values.astype(BF16)

    def project(i, _, last=False):
        slot = lax.rem(i, 2)
        rows = pl.ds(pl.multiple_of(i * tile, tile), tile)
        held = None
        done = 0
        for n, (w, at) in enumerate(steps):
            ref = (wq_ref, wk_ref, wv_ref)[w]
            values = jnp.dot(
                normed[slot], ref[:, at : at + step], preferred_element_type=F32
            )
            if held is not None:
                store(rows, *held)
            upto = strips * (n + 1) // len(steps)
            while done < upto and not last:
                norm_strip((i + 1) * tile, 1 - slot, done)
                done += 1
            held = (w, at, values)
        store(rows, *held)
        return 0

    lax.fori_loop(0, tiles - 1, project, 0)
    project(tiles - 1, 0, True)
    if take:
        starts = take(where_ref[0], where_ref[1])
        size = edge_ref.shape[0] // len(starts)
        for i, start in enumerate(starts):
            rows = pl.ds(pl.multiple_of(start, GRID_W), size)
            edge_ref[i * size : (i + 1) * size, :] = kv_ref[rows, :]


def qkv(
    where,
    pieces,
    mods,
    norm_gain,
    w_query,
    w_key,
    w_value,
    query_gain,
    key_gain,
    heads,
    take=None,
    taken=0,
):
    total = sum(p.shape[0] for p in pieces)
    depth, width = w_query.shape
    tile = 384 if total % 384 == 0 else 256 if total % 256 == 0 else 128
    outs = [
        jax.ShapeDtypeStruct((total, width), BF16),
        jax.ShapeDtypeStruct((total, 2 * width), BF16),
    ]
    if take:
        outs.append(jax.ShapeDtypeStruct((taken, 2 * width), BF16))
    return pl.pallas_call(
        functools.partial(qkv_kernel, len(pieces), heads, tile, take),
        out_shape=tuple(outs),
        in_specs=[SM] + [VM] * (len(pieces) + 8),
        out_specs=tuple(VM for _ in outs),
        scratch_shapes=[
            pltpu.VMEM((total, depth), BF16),
            pltpu.VMEM((2, tile, depth), BF16),
            pltpu.VMEM((2, depth), F32),
        ],
        name="qkv",
        compiler_params=params(24),
        cost_estimate=cost(6 * total * depth * width, total * depth * 2 + 6 * depth * width),
    )(
        where,
        *pieces,
        *mods,
        norm_gain.reshape(1, -1),
        w_query,
        w_key,
        w_value,
        query_gain.reshape(1, -1),
        key_gain.reshape(1, -1),
    )


def context_kernel(heads, x_ref, gain_ref, wk_ref, wv_ref, kg_ref, kv_ref):
    width = heads * HEAD_DIM
    floats = x_ref[...].astype(F32)
    inverse = lax.rsqrt(jnp.mean(floats * floats, axis=-1, keepdims=True) + EPS)
    x = (floats * inverse * gain_ref[...]).astype(BF16)
    kv_ref[:, :width] = normed_heads(
        jnp.dot(x, wk_ref[...], preferred_element_type=F32), kg_ref[...], heads
    )
    kv_ref[:, width:] = jnp.dot(x, wv_ref[...], preferred_element_type=F32).astype(BF16)


def context_kv(context, norm_gain, w_key, w_value, key_gain, heads):
    count, depth = context.shape
    width = w_key.shape[1]
    return pl.pallas_call(
        functools.partial(context_kernel, heads),
        out_shape=jax.ShapeDtypeStruct((count, 2 * width), BF16),
        in_specs=[VM] * 5,
        out_specs=VM,
        name="context_kv",
        compiler_params=params(16),
        cost_estimate=cost(4 * count * depth * width, 4 * depth * width),
    )(context, norm_gain.reshape(1, -1), w_key, w_value, key_gain.reshape(1, -1))


def attend_kernel(
    heads, span, groups, q_spec, kv_spec, n_ctx, rows_of, total, where_ref, cbias_ref, *refs
):
    n_q, n_kv = q_spec[-1][0] + 1, kv_spec[-1][0] + 1
    q_refs, refs = refs[:n_q], refs[n_q:]
    kv_refs, refs = refs[:n_kv], refs[n_kv:]
    ctx_refs, refs = refs[:n_ctx], refs[n_ctx:]
    tab_ref, out_ref, keys, queries, context, scores, weights = refs
    width = heads * HEAD_DIM
    block = span * GRID_W
    key_rows = span + WIN_ROWS
    window = key_rows * GRID_W
    ctx_count = context.shape[0]
    factor = LOG2E * HEAD_DIM**-0.5
    lines = 2 * GRID_W
    first, rows_at = rows_of(where_ref[0], where_ref[1])
    base = 0
    for i, (j, at, size) in enumerate(q_spec):
        to = pl.multiple_of(rows_at[base + i] * GRID_W, GRID_W)
        queries[pl.ds(to, size), :] = q_refs[j][at : at + size, :]
    base += len(q_spec)
    for i, (j, at, size) in enumerate(kv_spec):
        to = pl.multiple_of((rows_at[base + i] + REACH) * GRID_W, GRID_W)
        keys[pl.ds(to, size), :] = kv_refs[j][at : at + size, :]
    base += len(kv_spec)
    at = 0
    for ref in ctx_refs:
        context[at : at + ref.shape[0], :] = ref[...]
        at += ref.shape[0]
    nt = (((1,), (1,)), ((), ()))

    def group(i, _):
        row = rows_at[base] + i * span
        q_at = pl.multiple_of(row * GRID_W, GRID_W)
        top = first + row
        start = jnp.clip(top - REACH, 0, total - key_rows)
        k_at = pl.multiple_of((start - first + REACH) * GRID_W, GRID_W)
        spots = []
        for r in range(span):
            g = top + r
            a = jnp.clip(g - REACH, 0, total - WIN_ROWS)
            for p in range(key_rows // 2):
                u = start + 2 * p
                lv = (u >= a) & (u < a + WIN_ROWS)
                rv = (u + 1 >= a) & (u + 1 < a + WIN_ROWS)
                both = jnp.where(rv, u - g + WIN_ROWS - 1, BLANK - 2)
                spots.append(jnp.where(lv, both, jnp.where(rv, BLANK - 1, BLANK)))

        def score(h):
            hk = slice(h * HEAD_DIM, (h + 1) * HEAD_DIM)
            q = queries[pl.ds(q_at, block), hk]
            scores[h % 2, :, :window] = lax.dot_general(
                q, keys[pl.ds(k_at, window), hk], nt, preferred_element_type=F32
            )
            scores[h % 2, :, window:] = lax.dot_general(
                q, context[:, hk], nt, preferred_element_type=F32
            )

        def soften(h):
            cbias = cbias_ref[h] * LOG2E
            sums = []
            for r in range(span):
                for sub in range(GRID_W // LUMP):
                    rows = slice(r * GRID_W + sub * LUMP, r * GRID_W + (sub + 1) * LUMP)
                    lump = slice(sub * LUMP, (sub + 1) * LUMP)
                    tiles = []
                    for p in range(key_rows // 2):
                        cols = slice(p * lines, (p + 1) * lines)
                        bias = tab_ref[h, spots[r * (key_rows // 2) + p], lump, :]
                        tiles.append(scores[h % 2, rows, cols] * factor + bias)
                    for p in range(ctx_count // lines):
                        cols = slice(window + p * lines, window + (p + 1) * lines)
                        tiles.append(scores[h % 2, rows, cols] * factor + cbias)
                    tops = tiles
                    while len(tops) > 1:
                        tops = [
                            jnp.maximum(*tops[n : n + 2]) if n + 1 < len(tops) else tops[n]
                            for n in range(0, len(tops), 2)
                        ]
                    high = jnp.max(tops[0], axis=1, keepdims=True)
                    acc = None
                    for p, tile in enumerate(tiles):
                        tile = jnp.exp2(tile - high)
                        acc = tile if acc is None else acc + tile
                        weights[h % 2, rows, p * lines : (p + 1) * lines] = tile.astype(BF16)
                    sums.append(jnp.sum(acc, axis=1, keepdims=True))
            return sums

        def combine(h, sums):
            hk = slice(h * HEAD_DIM, (h + 1) * HEAD_DIM)
            hv = slice(width + h * HEAD_DIM, width + (h + 1) * HEAD_DIM)
            out = jnp.dot(
                weights[h % 2, :, :window], keys[pl.ds(k_at, window), hv], preferred_element_type=F32
            )
            out = out + jnp.dot(
                weights[h % 2, :, window:], context[:, hv], preferred_element_type=F32
            )
            out = (out / jnp.concatenate(sums, axis=0)).astype(BF16)
            out_ref[pl.ds(i * block if groups == 1 else pl.multiple_of(i * block, block), block), hk] = out

        score(0)
        held = None
        for h in range(heads):
            if h + 1 < heads:
                score(h + 1)
            sums = soften(h)
            if held is not None:
                combine(*held)
            held = (h, sums)
        combine(*held)
        return 0

    if groups == 1:
        group(0, 0)
    else:
        lax.fori_loop(0, groups, group, 0)


def attend(
    where, queries, q_spec, kvs, kv_spec, ctx, tables, context_bias, rows_of, total, span, groups, rows
):
    heads = tables.shape[0]
    width = heads * HEAD_DIM
    block = span * GRID_W
    ctx_count = sum(c.shape[0] for c in ctx)
    keys = (span + WIN_ROWS) * GRID_W + ctx_count
    elements = groups * block * heads * keys
    return pl.pallas_call(
        functools.partial(
            attend_kernel, heads, span, groups, q_spec, kv_spec, len(ctx), rows_of, total
        ),
        out_shape=jax.ShapeDtypeStruct((groups * block, width), BF16),
        in_specs=[SM, SM] + [VM] * (len(queries) + len(kvs) + len(ctx) + 1),
        out_specs=VM,
        scratch_shapes=[
            pltpu.VMEM(((rows + 2 * REACH) * GRID_W, 2 * width), BF16),
            pltpu.VMEM((rows * GRID_W, width), BF16),
            pltpu.VMEM((ctx_count, 2 * width), BF16),
            pltpu.VMEM((2, block, keys), F32),
            pltpu.VMEM((2, block, keys), BF16),
        ],
        name="attend",
        compiler_params=params(28),
        cost_estimate=cost(8 * elements * HEAD_DIM, 8 << 20, elements),
    )(where, context_bias, *queries, *kvs, *ctx, tables)


def out_kernel(masks, tile, where_ref, *refs):
    count = len(masks)
    pieces = refs[:count]
    w_ref, resid_ref, ma_ref, mb_ref, out_ref, held = refs[count:]
    depth = pieces[0].shape[1]
    width = w_ref.shape[1]
    for mask, piece in zip(masks, pieces):
        spot = pl.ds(pl.multiple_of(mask(where_ref[1]) * depth, depth), depth)
        held[:, spot] = piece[...]
    for n in range(width // tile):
        cols = slice(n * tile, (n + 1) * tile)
        total = jnp.dot(held[...], w_ref[:, cols], preferred_element_type=F32)
        spot = slice(2 * width + n * tile, 2 * width + (n + 1) * tile)
        gate = ma_ref[:, spot] + mb_ref[:, spot]
        out_ref[:, cols] = (resid_ref[:, cols].astype(F32) + gate * total).astype(BF16)


def out_project(where, pieces, masks, w_out, resid, mods):
    count, width = resid.shape
    depth = w_out.shape[0]
    tile = 512
    return pl.pallas_call(
        functools.partial(out_kernel, masks, tile),
        out_shape=jax.ShapeDtypeStruct((count, width), BF16),
        in_specs=[SM] + [VM] * len(pieces) + [VM, VM, VM, VM],
        out_specs=VM,
        scratch_shapes=[
            pltpu.VMEM((count, depth), BF16),
        ],
        name="out_project",
        compiler_params=params(16),
        cost_estimate=cost(2 * count * width * depth, 2 * depth * width + 8 * count * width),
    )(where, *pieces, w_out, resid, *mods)


def swap(count, bit):
    return [(i, i ^ bit) for i in range(count)]


def tie(value, other):
    return lax.optimization_barrier((value, other))[0]


def gather_context(where, ctx, bits, after):
    order = bits[-1:] + bits[:-1]
    for i, bit in enumerate(order):
        got = lax.ppermute(ctx, "sp", swap(lax.axis_size("sp"), bit))
        if i + 2 == len(order):
            return lambda value: gather_last(where, ctx, got, order[-1], value)
        ctx = join(ctx, tie(got, after), where)


def gather_last(where, ctx, got, bit, value):
    ctx = join(ctx, tie(got, value), where)
    return [ctx, lax.ppermute(ctx, "sp", swap(lax.axis_size("sp"), bit))]


def plain(where, resid, mods, norm_gain, ctx, tables, weights, gains, context_bias, w_out, heads):
    sp, tp = lax.axis_size("sp"), lax.axis_size("tp")
    own = resid.shape[0]
    tokens = own * tp
    rows = tokens // GRID_W
    piece = lax.all_gather(resid, "tp", axis=0, tiled=True)
    q, kv = qkv(where, [piece], mods, norm_gain, *weights, *gains, heads)
    ctx = ctx(kv)
    edge = REACH * GRID_W
    above = lax.ppermute(kv[tokens - edge :], "sp", [(i, i + 1) for i in range(sp - 1)])
    below = lax.ppermute(kv[:edge], "sp", [(i + 1, i) for i in range(sp - 1)])
    span = 4 if rows % 4 == 0 else 2
    attended = attend(
        where,
        [q],
        [(0, 0, tokens)],
        [kv, above, below],
        [(0, 0, tokens), (1, 0, edge), (2, 0, edge)],
        ctx,
        tables,
        context_bias,
        lambda s, t: (s * rows, [0, 0, -REACH, rows, 0]),
        sp * rows,
        span,
        rows // span,
        rows,
    )
    full = lax.all_to_all(attended.reshape(tp, own, -1), "tp", split_axis=0, concat_axis=0)
    masks = [lambda t, i=i: jnp.int32(i) for i in range(tp)]
    return out_project(where, [full[i] for i in range(tp)], masks, w_out, resid, mods)


CHUNKS = 3


def chunk_row(source, j, block_rows, chunk_rows):
    return source * block_rows + jnp.where(
        (source & 1) == 0, j * chunk_rows, block_rows - (j + 1) * chunk_rows
    )


def staged_tokens(where, resid):
    across = []
    for chunk in cut_chunks(where, resid, CHUNKS):
        across.append(lax.ppermute(chunk, "tp", swap(4, 2)))
    partner = lax.ppermute(resid, "tp", swap(4, 1))
    return partner, across


def staged(
    where, resid, mods, norm_gain, staged_in, ctx, tables, weights, gains, context_bias, w_out, heads
):
    sp, tp = lax.axis_size("sp"), lax.axis_size("tp")
    own = resid.shape[0]
    block_rows = own // GRID_W
    chunk_rows = block_rows // CHUNKS
    chunk = chunk_rows * GRID_W
    rows = block_rows * tp
    edge = REACH * GRID_W
    partner, across = staged_in
    project = functools.partial(
        qkv,
        where,
        mods=mods,
        norm_gain=norm_gain,
        w_query=weights[0],
        w_key=weights[1],
        w_value=weights[2],
        query_gain=gains[0],
        key_gain=gains[1],
        heads=heads,
    )

    def near_rows(t):
        return [t * block_rows, (t ^ 1) * block_rows]

    def chunk_rows_of(t, j):
        return [chunk_row(t ^ mask, j, block_rows, chunk_rows) for mask in (2, 3)]

    def early_at(s, t):
        chip, parity = t >> 1, t & 1
        return [jnp.where(chip == parity, 0, own) + jnp.where(chip == 0, 0, own - edge)]

    def late_at(s, t):
        at = jnp.where((t >> 1) + (t & 1) == 1, 0, chunk)
        return [at, at + 2 * chunk]

    down = [(s * tp + t, (s - 1) * tp + t) for s in range(1, sp) for t in range(tp)]
    up = [(s * tp + t, (s + 1) * tp + t) for s in range(sp - 1) for t in range(tp)]
    early = [p for p in down if p[0] % tp < 2] + [p for p in up if p[0] % tp >= 2]
    late = [p for p in up if p[0] % tp < 2] + [p for p in down if p[0] % tp >= 2]

    q0, kv0, edge_kv = project([resid, partner], take=early_at, taken=edge)
    ctx = ctx(kv0)
    early_kv = lax.ppermute(edge_kv, ("sp", "tp"), early)
    beside0 = lax.ppermute(across[0], "tp", swap(4, 1))
    beside1 = lax.ppermute(tie(across[1], kv0), "tp", swap(4, 1))
    q1, kv1, edge_kv = project(
        list(tie((across[0], beside0, across[1], beside1), kv0)), take=late_at, taken=2 * chunk
    )
    near = [(0, 0, own), (0, own, own)]
    pair = [(0, chunk), (chunk, chunk)]
    kv_spec = near + [(1, j * chunk, chunk) for j in range(4)] + [(2, at, size) for at, size in pair]

    def block(queries, q_spec, kvs, kv_spec, rows_of):
        return attend(
            where,
            queries,
            q_spec,
            kvs,
            kv_spec,
            ctx,
            tables,
            context_bias,
            rows_of,
            sp * rows,
            block_rows,
            1,
            rows,
        )

    def home_rows(last, late):
        def rows_of(s, t):
            chip = t >> 1
            at = near_rows(t) + near_rows(t) + chunk_rows_of(t, 0) + chunk_rows_of(t, 1)
            if late:
                for j in range(2):
                    at.append(jnp.where(chip == 0, -(j + 1) * chunk_rows, rows + j * chunk_rows))
            return s * rows, at + [last(chip) * block_rows]

        return rows_of

    beside2 = lax.ppermute(tie(across[2], kv0), "tp", swap(4, 1))
    q2, kv2 = project(list(tie((across[2], beside2), kv1)))

    def far(last, waits):
        outside = [] if waits is None else [jnp.where]

        def rows_of(s, t):
            chunks = [row for j in range(CHUNKS) for row in chunk_rows_of(t, j)]
            at = chunks + near_rows(t) + chunks
            at += [f(t < 2, rows, -REACH) for f in outside]
            return s * rows, at + [last(t >> 1) * block_rows]

        return block(
            [tie(q1, waits if outside else kv2), q2],
            [(j - 1, at, size) for j, at, size in kv_spec[2:]],
            [kv0, kv1, kv2] + [early_kv] * len(outside),
            kv_spec + [(3, 0, edge)] * len(outside),
            rows_of,
        )

    away2 = far(lambda chip: 2 - chip, None)
    first = lax.ppermute(away2, "tp", swap(4, 2))
    inner = block(
        [tie(q0, away2)], near, [kv0, kv1], kv_spec[:6], home_rows(lambda chip: 1 + chip, False)
    )
    late_kv = lax.ppermute(tie(edge_kv, away2), ("sp", "tp"), late)
    away3 = far(lambda chip: 3 - 3 * chip, inner)
    second = lax.ppermute(away3, "tp", swap(4, 2))
    outer = block(
        [tie(q0, away3)],
        near,
        [kv0, kv1, late_kv],
        kv_spec[:6] + [(2, at, size) for at, size in pair],
        home_rows(lambda chip: 3 * chip, True),
    )
    send, keep = pick(inner, outer, where)
    from_1 = lax.ppermute(send, "tp", swap(4, 1))
    send, kept = pick(first, tie(second, send), where)
    from_3 = lax.ppermute(send, "tp", swap(4, 1))
    masks = [lambda t, i=i: t ^ i for i in range(4)]
    return out_project(where, [keep, from_1, kept, from_3], masks, w_out, resid, mods)


def shards(
    resid,
    cond,
    mod_shift,
    mod_scale,
    mod_gate,
    norm_gain,
    context,
    w_query,
    w_key,
    w_value,
    query_gain,
    key_gain,
    offset_bias,
    context_bias,
    w_out,
):
    heads = offset_bias.shape[0]
    sp, tp = lax.axis_size("sp"), lax.axis_size("tp")
    block_rows = resid.shape[0] // GRID_W
    split = tp == 4 and sp == 8 and block_rows == CHUNKS * REACH // 2
    where = jnp.stack([lax.axis_index("sp"), lax.axis_index("tp")]).astype(jnp.int32)

    tables = bias_tables(offset_bias)
    parts = [mod_part(cond, mod_shift, mod_scale, mod_gate)]
    masks = [0]
    bit = tp // 2
    while bit:
        parts += [lax.ppermute(p, "tp", swap(tp, bit)) for p in parts]
        masks += [v ^ bit for v in masks]
        bit //= 2
    run = plain
    if split:
        run = functools.partial(staged, staged_in=staged_tokens(where, resid))
    mods = place_mods(parts, masks, where)
    bit = 1
    while bit < sp:
        other = lax.ppermute(mods, "sp", swap(sp, bit))
        bit *= 2
        if bit < sp:
            mods = add(mods, other, where)

    ctx = context_kv(context, norm_gain, w_key, w_value, key_gain, heads)
    bits = [1 << i for i in range(sp.bit_length() - 1)]
    ctx = gather_context(where, ctx, bits, other)
    return run(
        where,
        resid,
        (mods, other),
        norm_gain,
        ctx=ctx,
        tables=tables,
        weights=(w_query, w_key, w_value),
        gains=(query_gain, key_gain),
        context_bias=context_bias,
        w_out=w_out,
        heads=heads,
    )


def solution(mesh):
    in_specs = (
        P(("sp", "tp"), None),
        P("sp"),
        P("sp", "tp"),
        P("sp", "tp"),
        P("sp", "tp"),
        P(),
        P("sp", None),
        P(None, "tp"),
        P(None, "tp"),
        P(None, "tp"),
        P(),
        P(),
        P("tp", None, None),
        P("tp"),
        P(),
    )
    out_specs = P(("sp", "tp"), None)
    return jax.shard_map(shards, mesh=mesh, in_specs=in_specs, out_specs=out_specs, check_vma=False)
```
